32 devices in a mesh: rep: 4 (over z), fs: 2 (over y), tp: 4 (over x, core).
Axes of the slice: x: 2, y: 2, z: 4, core: 2. Of those that a mesh axis runs over, the one named last changes fastest.
Arguments:
- inputs: bfloat16 [2560, 2048], P('rep', 'fs'), may hold values from -6 to 6
- gate_pre: bfloat16 [2560, 5632], P('rep', 'tp'), may hold values from -12 to 12
- up_pre: bfloat16 [2560, 5632], P('rep', 'tp'), may hold values from -6 to 6
- cotangent: bfloat16 [2560, 2048], P('rep'), may hold values from -6 to 6
- w_gate: bfloat16 [2048, 5632], P('fs', 'tp'), may hold values from -0.125 to 0.125
- w_up: bfloat16 [2048, 5632], P('fs', 'tp'), may hold values from -0.125 to 0.125
- w_down: bfloat16 [5632, 2048], P('tp', 'fs'), may hold values from -0.078125 to 0.078125
Outputs:
- grad_input: bfloat16 [2560, 2048], P('rep', 'fs')
- grad_gate: float32 [512, 4, 5632], P('fs', 'rep', 'tp')
- grad_up: float32 [512, 4, 5632], P('fs', 'rep', 'tp')
- grad_down: float32 [5632, 512, 4], P('tp', 'fs', 'rep')
- gate_norms: float32 [512, 4], P('fs', 'rep')
- up_norms: float32 [512, 4], P('fs', 'rep')
- down_norms: float32 [5632], P('tp')
The draws below stay inside these ranges and needn't reach their ends.
All inputs are finite; a program needn't handle non-finite values.
Results may differ from the reference program's by a relative error of at most 0.02.
Values may be sent and summed in bfloat16 or wider, within the bound.
A program may use at most 64 MiB of HBM per device.

```python
import jax
import jax.numpy as jnp
from jax import lax

D = 2048
FF = 5632
TOKENS = 2560
N_REP = 4
N_TP = 4


def raised(values, key, source, target, shards_of, factor):
    def block_of(position):
        return (jnp.arange(values.shape[position]) // (values.shape[position] // shards_of)).reshape((-1,) + (1,) * (values.ndim - 1 - position))

    first = jax.random.permutation(key, shards_of)[block_of(target)]
    far = (block_of(target) + shards_of // 2) % shards_of
    return jnp.where((block_of(source) == first) | (block_of(source) == far), factor * values, values)


def level_of(own_key, shape, pieces, smallest, high):
    def one(dim, blocks):
        heights = jax.random.uniform(jax.random.fold_in(jax.random.fold_in(own_key, 6), dim), (blocks,), jnp.float32, smallest / len(pieces), high / len(pieces))
        return jnp.repeat(jnp.exp(heights), shape[dim] // blocks).reshape((-1,) + (1,) * (len(shape) - dim - 1))

    level = one(*pieces[0])
    for cut in pieces[1:]:
        level = level * one(*cut)
    return level


def bell_draw(own_key, shape, scale, bound, shards=(), kind=jnp.bfloat16):
    loudness = level_of(own_key, shape, shards, -0.22, 0.18) if shards else 1.0
    drawn = jax.random.normal(own_key, shape, jnp.float32) * scale * loudness
    return jnp.minimum(jnp.maximum(drawn, -bound), bound).astype(kind)


def heavy_noise(key, extent, deviation, most, pieces, heavy, held_as=jnp.bfloat16):
    entries = deviation * jax.random.normal(key, extent, jnp.float32)
    if pieces:
        entries = entries * level_of(key, extent, pieces, -0.22, 0.18)
    return jnp.clip(raised(entries, jax.random.fold_in(key, 3), *heavy), -most, most).astype(held_as)


def setup_inputs(seed: int = 0) -> dict:
    streams_of = jax.random.split(jax.random.key(seed), 8)
    return {
        "inputs": bell_draw(streams_of[0], (TOKENS, D), 1.0, 6.0, ((0, 4), (1, 2))),
        "gate_pre": bell_draw(streams_of[1], (TOKENS, FF), 2.0, 12.0, ((0, 4), (1, 4))),
        "up_pre": bell_draw(streams_of[2], (TOKENS, FF), 1.0, 6.0, ((0, 4), (1, 4))),
        "cotangent": heavy_noise(streams_of[3], (TOKENS, D), 1.0, 6.0, ((0, 4),), (0, 1, 4, 2.0)),
        "w_gate": bell_draw(streams_of[4], (D, FF), D ** -0.5, 0.125, ((0, 2), (1, 4))),
        "w_up": bell_draw(streams_of[5], (D, FF), D ** -0.5, 0.125, ((0, 2), (1, 4))),
        "w_down": bell_draw(streams_of[6], (FF, D), FF ** -0.5, 0.078125, ((0, 4), (1, 2))),
    }


def reference(inputs, gate_pre, up_pre, cotangent, w_gate, w_up, w_down):
    single = jnp.float32
    hidden_grad = jnp.dot(cotangent, w_down.T, preferred_element_type=single)
    gate = gate_pre.astype(single)
    upper = up_pre.astype(single)
    sigma = jax.nn.sigmoid(gate)
    active = gate * sigma
    hidden = (active * upper).astype(jnp.bfloat16)
    d_up = (hidden_grad * active).astype(jnp.bfloat16)
    d_gate = (hidden_grad * upper * sigma * (1.0 + gate * (1.0 - sigma))).astype(jnp.bfloat16)
    factor = float(TOKENS) ** -0.5
    grad_gate = jnp.dot(inputs.T, d_gate, preferred_element_type=single) * factor
    grad_up = jnp.dot(inputs.T, d_up, preferred_element_type=single) * factor
    grad_down = jnp.dot(hidden.T, cotangent, preferred_element_type=single) * factor
    block = FF // N_TP
    total = jnp.zeros(inputs.shape, single)
    for index in range(N_TP):
        lower = index * block
        term = jnp.dot(d_gate[:, lower:lower + block], w_gate[:, lower:lower + block].T, preferred_element_type=single)
        term = term + jnp.dot(d_up[:, lower:lower + block], w_up[:, lower:lower + block].T, preferred_element_type=single)
        term = lax.optimization_barrier(term.astype(jnp.bfloat16)).astype(single)
        total = total + term
    grad_input = total.astype(jnp.bfloat16)
    gate_norms = jnp.sum(grad_gate * grad_gate, axis=1).reshape(D // N_REP, N_REP)
    up_norms = jnp.sum(grad_up * grad_up, axis=1).reshape(D // N_REP, N_REP)
    down_norms = jnp.sum(grad_down * grad_down, axis=1)
    return (grad_input, grad_gate.reshape(D // N_REP, N_REP, FF), grad_up.reshape(D // N_REP, N_REP, FF),
            grad_down.reshape(FF, D // N_REP, N_REP), gate_norms, up_norms, down_norms)
```

```python
import functools

import jax
import jax.numpy as jnp
from jax import lax
from jax.experimental import pallas as pl
from jax.experimental.pallas import tpu as pltpu
from jax.sharding import PartitionSpec as P

LANES = 128
CHUNK = 256
LATE = 4
VMEM_LIMIT = 56 * 2**20
F32 = jnp.float32
BF16 = jnp.bfloat16
MESH = pl.DeviceIdType.MESH
NT = (((1,), (1,)), ((), ()))


def on_device(inputs, gate_pre, up_pre, cotangent, w_gate, w_up, w_down):
    single = jnp.float32
    groups = lax.axis_size("rep")
    width = w_down.shape[1]
    own_cot = lax.dynamic_slice_in_dim(cotangent, lax.axis_index("fs") * width, width, 1)
    partial_grad = jnp.einsum("td,fd->tf", own_cot, w_down, preferred_element_type=single)
    hidden_grad = lax.psum(partial_grad.astype(jnp.bfloat16), "fs").astype(jnp.float32)
    gate = gate_pre.astype(single)
    upper = up_pre.astype(single)
    sigma = jax.nn.sigmoid(gate)
    active = gate * sigma
    hidden = (active * upper).astype(jnp.bfloat16)
    d_up = (hidden_grad * active).astype(jnp.bfloat16)
    d_gate = (hidden_grad * upper * sigma * (1.0 + gate * (1.0 - sigma))).astype(jnp.bfloat16)
    factor = float(inputs.shape[0] * groups) ** (-0.5)
    owned = width // groups
    hunits = w_gate.shape[1]
    gate_local = jnp.einsum("td,tf->df", inputs, d_gate, preferred_element_type=single) * factor
    gate_parts = lax.all_to_all(
        gate_local.reshape(owned, groups, hunits).astype(jnp.bfloat16),
        "rep",
        split_axis=1,
        concat_axis=1,
        tiled=True,
    ).astype(jnp.float32)
    grad_gate = jnp.sum(gate_parts, axis=1, keepdims=True)
    up_local = jnp.einsum("td,tf->df", inputs, d_up, preferred_element_type=single) * factor
    up_parts = lax.all_to_all(
        up_local.reshape(owned, groups, hunits).astype(jnp.bfloat16),
        "rep",
        split_axis=1,
        concat_axis=1,
        tiled=True,
    ).astype(jnp.float32)
    grad_up = jnp.sum(up_parts, axis=1, keepdims=True)
    down_local = jnp.einsum("tf,td->fd", hidden, own_cot, preferred_element_type=single) * factor
    down_parts = lax.all_to_all(
        down_local.reshape(hunits, owned, groups).astype(jnp.bfloat16),
        "rep",
        split_axis=2,
        concat_axis=2,
        tiled=True,
    ).astype(jnp.float32)
    grad_down = jnp.sum(down_parts, axis=2, keepdims=True)
    input_term = jnp.einsum("tf,df->td", d_gate, w_gate, preferred_element_type=single)
    input_term = input_term + jnp.einsum("tf,df->td", d_up, w_up, preferred_element_type=single)
    grad_input = lax.psum(input_term.astype(jnp.bfloat16), "tp")
    gate_norms, up_norms = lax.psum(
        (jnp.sum(grad_gate * grad_gate, axis=2), jnp.sum(grad_up * grad_up, axis=2)), "tp"
    )
    down_norms = lax.psum(jnp.sum(grad_down * grad_down, axis=(1, 2)), ("rep", "fs"))
    return (grad_input, grad_gate, grad_up, grad_down, gate_norms, up_norms, down_norms)


def line_kernel(
    sizes, x_hbm, gate_hbm, up_hbm, cot_hbm, wg_hbm, wu_hbm, wd_hbm,
    gi_ref, gate_out, up_out, down_out, gu_norm_ref, down_norm_ref,
    x_ref, gate_ref, up_ref, cot_ref, wg_ref, wu_ref, wd_ref,
    left, left_far, right, right_far, pg_own, pg_peer, ab, sb, bb, gi_acc, gi_own, gi_peer,
    squares, gu_own, gu_peer, dn_own, dn_peer,
    load_sem, y_send, y_recv, a_send, a_recv, b_send, b_recv, c_send, c_recv,
    r_send, r_recv, f_send, f_recv, l_send, l_recv, m_send, m_recv,
    gi_send, gi_recv, gg_send, gg_recv, gn_send, gn_recv, dn_send, dn_recv,
):
    n_fs, n_tp, factor = sizes
    tokens, width = x_ref.shape
    hunits = gate_ref.shape[1]
    blocks = hunits // LANES
    owned = width // 4
    share = tokens // n_tp
    rep, fs, tp = lax.axis_index("rep"), lax.axis_index("fs"), lax.axis_index("tp")
    side = rep // 2
    mid, end = 1 + side, 3 * side
    far_mid, far_end = 2 - side, 3 - 3 * side
    at_end = rep == end
    partner = mid + end - rep
    fs_peer = 1 - fs
    tp_next = tp + 1 - 2 * lax.rem(tp, 2)
    tp_far = lax.rem(tp + 2, n_tp)

    loads = [
        pltpu.make_async_copy(cot_hbm.at[:, pl.ds(pl.multiple_of(fs * width, LANES), width)], cot_ref, load_sem.at[0]),
        pltpu.make_async_copy(wd_hbm, wd_ref, load_sem.at[1]),
        pltpu.make_async_copy(gate_hbm, gate_ref, load_sem.at[2]),
        pltpu.make_async_copy(up_hbm, up_ref, load_sem.at[3]),
        pltpu.make_async_copy(x_hbm, x_ref, load_sem.at[4]),
        pltpu.make_async_copy(wg_hbm, wg_ref, load_sem.at[5]),
        pltpu.make_async_copy(wu_hbm, wu_ref, load_sem.at[6]),
    ]
    for k in (4, 0, 1, 2, 3, 5, 6):
        loads[k].start()

    group = [(r, f) for r in range(4) for f in range(n_fs) if r or f]

    def in_group(step):
        return (lax.rem(rep + step[0], 4), lax.rem(fs + step[1], n_fs), tp)

    def in_tp(step):
        return (rep, fs, lax.rem(tp + step, n_tp))

    barrier = pltpu.get_barrier_semaphore()
    greeted = [in_group(s) for s in group] + [in_tp(s) for s in range(1, n_tp)]
    for other in greeted:
        pl.semaphore_signal(barrier, inc=1, device_id=other, device_id_type=MESH)

    def remote(src, dst, send, recv, other):
        return pltpu.make_async_remote_copy(
            src_ref=src, dst_ref=dst, send_sem=send, recv_sem=recv, device_id=other, device_id_type=MESH
        )

    def rows_of(slot):
        return slice(slot * owned, (slot + 1) * owned)

    def y_copy(j):
        return remote(pg_own.at[j], pg_peer.at[j], y_send.at[j], y_recv.at[j], (rep, fs_peer, tp))

    def a_copy(t, late):
        piece = ab.at[t, pl.ds(0, owned) if late else pl.ds(owned, 2 * owned)]
        k = blocks * late + t
        return remote(piece, piece, a_send.at[k], a_recv.at[k], (partner, fs, tp))

    def b_copy(kind, t):
        src = ab.at[t, pl.ds(owned, 2 * owned)] if kind == 0 else sb.at[t - blocks]
        return remote(src, bb.at[t], b_send.at[t], b_recv.at[t], (far_mid, fs, tp))

    def c_copy(t):
        return remote(
            bb.at[t, pl.ds(owned, owned)], bb.at[t, pl.ds(0, owned)], c_send.at[t], c_recv.at[t], (partner, fs, tp)
        )

    half = tokens // n_fs
    own_half = pl.ds(pl.multiple_of(fs * half, 16), half)

    def r_copy(q):
        return remote(
            right.at[blocks + q, own_half], right_far.at[q, own_half], r_send.at[q], r_recv.at[q], (partner, fs, tp)
        )

    def f_copy(q):
        piece = right_far.at[q, own_half]
        return remote(piece, piece, f_send.at[q], f_recv.at[q], (rep, fs_peer, tp))

    piece_rows = owned // n_tp

    def piece_of(slot, owner):
        return pl.ds(pl.multiple_of(slot * owned + owner * piece_rows, 16), piece_rows)

    def l_copy(slot):
        rows = piece_of(slot, tp)
        return remote(left.at[1, rows], left_far.at[rows], l_send.at[slot], l_recv.at[slot], (partner, fs, tp))

    def m_copy(slot, hop):
        piece = left_far.at[piece_of(slot, tp_far if hop == 2 else tp)]
        k = 3 * slot + hop
        return remote(piece, piece, m_send.at[k], m_recv.at[k], (rep, fs, tp_next if hop else tp_far))

    def lanes(j):
        return pl.ds(pl.multiple_of(j * LANES, LANES), LANES)

    def term(kind, first, last, t):
        rows = slice(first * owned, last * owned)
        return jnp.dot(left[kind, rows, :], right[t], preferred_element_type=F32) * factor

    def long_term(first, last, t):
        rows = slice(first * owned, last * owned)
        own = jnp.dot(left[1, rows, :], right[t], preferred_element_type=F32)
        far = jnp.dot(left_far[rows, :], right_far[t - blocks], preferred_element_type=F32)
        return (own + far) * factor

    def loop(first, last, body):
        def step(i, carry):
            body(i)
            return carry
        lax.fori_loop(first, last, step, 0)

    def spread(kind, source):
        rows = CHUNK // 4
        lane = lax.broadcasted_iota(jnp.int32, (rows, CHUNK), 1)
        place = lax.broadcasted_iota(jnp.int32, (rows, CHUNK), 0) * 4
        pick = jnp.concatenate(
            [(place + owner == lane).astype(F32).astype(BF16) for owner in (mid, far_mid, far_end, end)], axis=0
        )
        for c in range(width // CHUNK):
            picked = lax.dot_general(
                pick, source[:, c * CHUNK:(c + 1) * CHUNK], NT, preferred_element_type=F32
            ).astype(BF16)
            for slot in range(4):
                left[kind, slot * owned + c * rows:slot * owned + (c + 1) * rows, :] = picked[slot * rows:(slot + 1) * rows]

    def item(kind, j):
        return j if kind == 0 else blocks + 2 * j + kind - 1

    def hidden_of(j):
        g = gate_ref[:, lanes(j)].astype(F32)
        u = up_ref[:, lanes(j)].astype(F32)
        right[j] = (g * (1.0 / (1.0 + jnp.exp(-g))) * u).astype(BF16)

    def send_down(t):
        ab[t] = term(0, 0, 3, t).astype(BF16)
        a_copy(t, 0).start()

    def partial_of(j):
        rows = pl.ds(pl.multiple_of(j * LANES, LANES), LANES)
        pg_own[j] = lax.dot_general(cot_ref[...], wd_ref[rows, :], NT, preferred_element_type=F32).astype(BF16)

    def partial_out(j):
        partial_of(j)
        y_copy(j).start()

    def grads_of(j):
        y_copy(j).wait_recv()
        g = gate_ref[:, lanes(j)].astype(F32)
        u = up_ref[:, lanes(j)].astype(F32)
        total = pg_own[j].astype(F32) + pg_peer[j].astype(F32)
        s = 1.0 / (1.0 + jnp.exp(-g))
        t = blocks + 2 * j
        right[t] = (total * u * s * (1.0 + g * (1.0 - s))).astype(BF16)
        right[t + 1] = (total * (g * s)).astype(BF16)

    def finish(kind, j, piece):
        if kind == 0:
            dn_own[0:1, lanes(j)] = jnp.sum(piece * piece, axis=0, keepdims=True)
            down_out[pl.ds(pl.multiple_of(j * LANES, LANES), LANES), 0, :] = piece.T
        else:
            squares[kind - 1] += piece * piece
            (gate_out if kind == 1 else up_out)[:, 0, lanes(j)] = piece

    def down_on(t):
        a_copy(t, 0).wait_recv()
        rows = slice(owned, 3 * owned)
        ab[t, rows, :] = (ab[t, rows, :].astype(F32) + term(0, 1, 3, t)).astype(BF16)
        b_copy(0, t).start()

    def forward(q):
        r_copy(q).wait_recv()
        f_copy(q).start()

    def pair_on(kind, j):
        t = item(kind, j)
        f_copy(t - blocks).wait_recv()
        sb[t - blocks] = long_term(1, 3, t).astype(BF16)
        b_copy(kind, t).start()

    def settle(kind, j):
        t = item(kind, j)
        b_copy(kind, t).wait_recv()
        bb[t, owned:, :] = (bb[t, owned:, :].astype(F32) + term(min(kind, 1), 3, 4, t)).astype(BF16)
        c_copy(t).start()
        if kind:
            finish(kind, j, long_term(0, 1, t) + bb[t, :owned, :].astype(F32))

    def settle_own(j):
        a_copy(j, 1).wait_recv()
        finish(0, j, ab[j, :owned, :].astype(F32) + term(0, 0, 1, j) + bb[j, :owned, :].astype(F32))

    def last_hop(kind, j):
        t = item(kind, j)
        c_copy(t).wait_recv()
        finish(kind, j, bb[t, :owned, :].astype(F32) + term(min(kind, 1), 3, 4, t))

    def gi_term(j):
        t = blocks + 2 * j
        gi_acc[...] += lax.dot_general(right[t], wg_ref[:, lanes(j)], NT, preferred_element_type=F32) + lax.dot_general(
            right[t + 1], wu_ref[:, lanes(j)], NT, preferred_element_type=F32
        )

    def grads_and_term(j):
        grads_of(j)
        gi_term(j)

    def tokens_of(owner):
        return pl.ds(pl.multiple_of(owner * share, share), share)

    def gi_copy(step):
        other = lax.rem(tp + step, n_tp)
        return remote(
            gi_own.at[tokens_of(other)], gi_peer.at[step - 1], gi_send.at[step - 1], gi_recv.at[step - 1], in_tp(step)
        )

    def gg_copy(hop):
        piece = gi_ref.at[tokens_of(tp_far if hop == 2 else tp)]
        return remote(piece, piece, gg_send.at[hop], gg_recv.at[hop], (rep, fs, tp_next if hop else tp_far))

    def gi_out():
        gi_own[...] = gi_acc[...].astype(BF16)
        for step in range(1, n_tp):
            gi_copy(step).start()

    def gi_sum():
        for step in range(1, n_tp):
            gi_copy(step).wait_recv()
        whole = gi_own[tokens_of(tp), :].astype(F32)
        for step in range(1, n_tp):
            whole += gi_peer[step - 1].astype(F32)
        gi_ref[tokens_of(tp), :] = whole.astype(BF16)
        gg_copy(0).start()
        gg_copy(1).start()

    def gi_pass():
        gg_copy(0).wait_recv()
        gg_copy(2).start()

    def dn_copy(k):
        return remote(dn_own, dn_peer.at[k], dn_send.at[k], dn_recv.at[k], in_group(group[k]))

    def dn_out():
        for k in range(len(group)):
            dn_copy(k).start()

    def gn_copy(step):
        return remote(gu_own, gu_peer.at[step - 1], gn_send.at[step - 1], gn_recv.at[step - 1], in_tp(step))

    loads[4].wait()
    spread(1, x_ref)
    pl.semaphore_wait(barrier, len(greeted))

    @pl.when(at_end)
    def _():
        l_copy(1).start()
        l_copy(2).start()

    loads[0].wait()
    loads[1].wait()
    loop(0, 1, partial_out)
    spread(0, cot_ref)
    loads[2].wait()
    loads[3].wait()

    @pl.when(at_end)
    def _():
        def out(j):
            hidden_of(j)
            send_down(j)

        def pair_out(j):
            grads_of(j)
            r_copy(2 * j).start()
            r_copy(2 * j + 1).start()

        loop(0, 1, out)
        loop(1, 6, partial_out)
        gi_acc[...] = jnp.zeros_like(gi_acc)

        def both_out(j):
            pair_out(j)
            out(j + 1)

            @pl.when(j == 1)
            def _():
                l_copy(0).start()

            @pl.when(j >= LATE)
            def _():
                a_copy(j - LATE, 1).start()

        loop(0, 1, both_out)
        loop(6, blocks, partial_out)
        loop(1, blocks - 1, both_out)
        pair_out(blocks - 1)
        loop(blocks - 1 - LATE, blocks, lambda t: a_copy(t, 1).start())
        squares[...] = jnp.zeros_like(squares)
        loads[5].wait()
        loads[6].wait()
        loop(0, blocks, gi_term)
        gi_out()

        def hops(j):
            last_hop(0, j - 1)
            last_hop(1, j - 2)
            last_hop(2, j - 2)

        last_hop(0, 0)
        loop(2, blocks - 3, hops)
        gi_sum()
        loop(blocks - 3, blocks, hops)
        last_hop(0, blocks - 1)
        dn_out()
        gi_pass()
        for j in (blocks - 2, blocks - 1):
            last_hop(1, j)
            last_hop(2, j)

    @pl.when(jnp.logical_not(at_end))
    def _():
        loop(1, 2, partial_out)
        loop(2, 6, partial_of)
        for slot in (1, 2):
            l_copy(slot).wait_recv()
            m_copy(slot, 0).start()
            m_copy(slot, 1).start()
        loop(6, blocks, partial_of)
        loop(0, blocks, hidden_of)
        down_on(0)
        grads_of(0)
        for slot in (1, 2):
            m_copy(slot, 0).wait_recv()
            m_copy(slot, 2).start()
        forward(0)
        gi_acc[...] = jnp.zeros_like(gi_acc)
        squares[...] = jnp.zeros_like(squares)
        loads[5].wait()
        loads[6].wait()
        forward(1)
        y_copy(2).start()
        for slot in (1, 2):
            m_copy(slot, 1).wait_recv()
            m_copy(slot, 2).wait_recv()
        pair_on(1, 0)
        down_on(1)
        pair_on(2, 0)
        grads_and_term(1)

        def first_y(j):
            return j + 2 + jnp.where(j > 3, 1, 0) + jnp.where(j > 5, 1, 0)

        def step(j, late):
            forward(2 * j)
            forward(2 * j + 1)
            if not late:
                new, old = first_y(j), first_y(j - 1)
                for extra in range(2):
                    @pl.when(jnp.logical_and(new + extra < blocks, extra == 0 if extra == 0 else jnp.logical_or(j == 3, j == 5)))
                    def _():
                        y_copy(new + extra).start()
                for extra in range(2):
                    @pl.when(jnp.logical_and(old + extra < blocks, extra == 0 if extra == 0 else jnp.logical_or(j == 4, j == 6)))
                    def _():
                        grads_and_term(old + extra)
            pair_on(1, j)
            pair_on(2, j)

        def early_step(j):
            step(j, False)
            down_on(j + 1)

        loop(1, 2, early_step)
        gi_term(0)
        l_copy(0).wait_recv()
        m_copy(0, 0).start()
        m_copy(0, 1).start()
        settle(0, 0)
        m_copy(0, 0).wait_recv()
        m_copy(0, 2).start()

        def settles(j):
            settle(0, j - 1)
            settle(1, j - 2)
            settle(2, j - 2)

            @pl.when(j >= LATE + 1)
            def _():
                settle_own(j - LATE - 1)

        loop(2, 3, early_step)
        m_copy(0, 1).wait_recv()
        m_copy(0, 2).wait_recv()

        def both(j):
            settles(j - 1)
            early_step(j)

        loop(3, blocks - 3, both)
        gi_out()

        def late_both(j):
            settles(j - 1)
            step(j, True)
            down_on(j + 1)

        loop(blocks - 3, blocks - 1, late_both)
        gi_sum()
        settles(blocks - 2)
        step(blocks - 1, True)
        settles(blocks - 1)
        gi_pass()
        loop(blocks - 1 - LATE, blocks - 1, settle_own)
        settle(0, blocks - 1)
        settle_own(blocks - 1)
        dn_out()
        for j in (blocks - 2, blocks - 1):
            settle(1, j)
            settle(2, j)

    for kind in range(2):
        gu_own[0:1, kind * owned:(kind + 1) * owned] = jnp.sum(squares[kind].T, axis=0, keepdims=True)
    for step in range(1, n_tp):
        gn_copy(step).start()

    for k in range(len(group)):
        dn_copy(k).wait_recv()
    down = dn_own[...]
    for k in range(len(group)):
        down += dn_peer[k]
    down_norm_ref[...] = down

    gg_copy(1).wait_recv()
    gg_copy(2).wait_recv()
    for step in range(1, n_tp):
        gg_copy(step - 1).wait_send()
        gi_copy(step).wait_send()
    for k in range(len(group)):
        dn_copy(k).wait_send()
    loop(0, blocks, lambda j: y_copy(j).wait_send())

    @pl.when(at_end)
    def _():
        for slot in range(3):
            l_copy(slot).wait_send()
        loop(0, blocks, lambda t: a_copy(t, 0).wait_send())
        loop(0, blocks, lambda t: a_copy(t, 1).wait_send())
        loop(0, 2 * blocks, lambda q: r_copy(q).wait_send())

    @pl.when(jnp.logical_not(at_end))
    def _():
        for slot in range(3):
            for hop in range(3):
                m_copy(slot, hop).wait_send()
        loop(0, blocks, lambda t: b_copy(0, t).wait_send())
        loop(blocks, 3 * blocks, lambda t: b_copy(1, t).wait_send())
        loop(0, 3 * blocks, lambda t: c_copy(t).wait_send())
        loop(0, 2 * blocks, lambda q: f_copy(q).wait_send())

    for step in range(1, n_tp):
        gn_copy(step).wait_recv()
    gate_up = gu_own[...]
    for step in range(1, n_tp):
        gate_up += gu_peer[step - 1]
    gu_norm_ref[...] = gate_up
    for step in range(1, n_tp):
        gn_copy(step).wait_send()


def store_kernel(gi_ref, gate_ref, up_ref, down_ref, gu_ref, dn_ref, *rest):
    sem, outs = rest[-1], rest[:-1]
    owned = gu_ref.shape[1] // 2
    sources = (
        gate_ref, up_ref, down_ref, gi_ref, gu_ref.at[:, pl.ds(0, owned)], gu_ref.at[:, pl.ds(owned, owned)], dn_ref
    )
    copies = [pltpu.make_async_copy(src, dst, sem.at[k]) for k, (src, dst) in enumerate(zip(sources, outs))]
    for copy in copies:
        copy.start()
    for copy in copies:
        copy.wait()


def on_line(inputs, gate_pre, up_pre, cotangent, w_gate, w_up, w_down):
    n_fs, n_tp = lax.axis_size("fs"), lax.axis_size("tp")
    tokens, width = inputs.shape
    hunits = w_gate.shape[1]
    blocks = hunits // LANES
    items = 3 * blocks
    owned = width // 4
    share = tokens // n_tp
    n_group = 4 * n_fs - 1
    dma = pltpu.SemaphoreType.DMA
    vmem = pltpu.VMEM
    sizes = (n_fs, n_tp, float(tokens * 4) ** (-0.5))
    shaped = jax.ShapeDtypeStruct
    gi_shape = shaped((tokens, width), BF16)
    row_shape = shaped((owned, 1, hunits), F32)
    down_shape = shaped((hunits, 1, owned), F32)
    results = pl.pallas_call(
        functools.partial(line_kernel, sizes),
        out_shape=(
            vmem((tokens, width), BF16),
            vmem((owned, 1, hunits), F32),
            vmem((owned, 1, hunits), F32),
            vmem((hunits, 1, owned), F32),
            vmem((1, 2 * owned), F32),
            vmem((1, hunits), F32),
        ),
        in_specs=[pl.BlockSpec(memory_space=pltpu.HBM)] * 7,
        out_specs=(pl.BlockSpec(memory_space=vmem),) * 6,
        scratch_shapes=[
            vmem((tokens, width), BF16),
            vmem((tokens, hunits), BF16),
            vmem((tokens, hunits), BF16),
            vmem((tokens, width), BF16),
            vmem((width, hunits), BF16),
            vmem((width, hunits), BF16),
            vmem((hunits, width), BF16),
            vmem((2, width, tokens), BF16),
            vmem((3 * owned, tokens), BF16),
            vmem((items, tokens, LANES), BF16),
            vmem((2 * blocks, tokens, LANES), BF16),
            vmem((blocks, tokens, LANES), BF16),
            vmem((blocks, tokens, LANES), BF16),
            vmem((blocks, 3 * owned, LANES), BF16),
            vmem((2 * blocks, 2 * owned, LANES), BF16),
            vmem((items, 2 * owned, LANES), BF16),
            vmem((tokens, width), F32),
            vmem((tokens, width), BF16),
            vmem((n_tp - 1, share, width), BF16),
            vmem((2, owned, LANES), F32),
            vmem((1, 2 * owned), F32),
            vmem((n_tp - 1, 1, 2 * owned), F32),
            vmem((1, hunits), F32),
            vmem((n_group, 1, hunits), F32),
            dma((7,)),
            dma((blocks,)), dma((blocks,)),
            dma((2 * blocks,)), dma((2 * blocks,)),
            dma((items,)), dma((items,)),
            dma((items,)), dma((items,)),
            dma((2 * blocks,)), dma((2 * blocks,)),
            dma((2 * blocks,)), dma((2 * blocks,)),
            dma((3,)), dma((3,)),
            dma((9,)), dma((9,)),
            dma((n_tp - 1,)), dma((n_tp - 1,)),
            dma((n_tp - 1,)), dma((n_tp - 1,)),
            dma((n_tp - 1,)), dma((n_tp - 1,)),
            dma((n_group,)), dma((n_group,)),
        ],
        compiler_params=pltpu.CompilerParams(
            collective_id=0, has_side_effects=True, vmem_limit_bytes=VMEM_LIMIT
        ),
    )(inputs, gate_pre, up_pre, cotangent, w_gate, w_up, w_down)
    grad_gate, grad_up, grad_down, grad_input, gate_norms, up_norms, down_norms = pl.pallas_call(
        store_kernel,
        out_shape=(
            row_shape, row_shape, down_shape, gi_shape,
            shaped((1, owned), F32), shaped((1, owned), F32), shaped((1, hunits), F32),
        ),
        in_specs=[pl.BlockSpec(memory_space=vmem)] * 6,
        out_specs=(pl.BlockSpec(memory_space=pltpu.HBM),) * 7,
        scratch_shapes=[dma((7,))],
        compiler_params=pltpu.CompilerParams(vmem_limit_bytes=2**23),
    )(*results)
    return (
        grad_input,
        grad_gate,
        grad_up,
        grad_down.transpose(0, 2, 1),
        gate_norms.reshape(owned, 1),
        up_norms.reshape(owned, 1),
        down_norms.reshape(hunits),
    )


def fits_line(mesh, inputs, w_gate):
    n_rep, n_fs, n_tp = (mesh.shape[axis] for axis in ("rep", "fs", "tp"))
    tokens, width = inputs.shape[0] // n_rep, inputs.shape[1] // n_fs
    return (
        n_rep == 4 and n_fs == 2 and n_tp == 4 and w_gate.shape[1] // n_tp >= 10 * LANES
        and width % (4 * LANES) == 0
        and tokens % (16 * n_tp) == 0 and tokens % LANES == 0
        and (w_gate.shape[1] // n_tp) % LANES == 0
    )


def solution(mesh):
    placed = (
        P("rep", "fs"),
        P("rep", "tp"),
        P("rep", "tp"),
        P("rep", None),
        P("fs", "tp"),
        P("fs", "tp"),
        P("tp", "fs"),
    )
    out_placed = (
        P("rep", "fs"),
        P("fs", "rep", "tp"),
        P("fs", "rep", "tp"),
        P("tp", "fs", "rep"),
        P("fs", "rep"),
        P("fs", "rep"),
        P("tp"),
    )

    def whole(inputs, gate_pre, up_pre, cotangent, w_gate, w_up, w_down):
        body = on_line if fits_line(mesh, inputs, w_gate) else on_device
        mapped = jax.shard_map(body, mesh=mesh, in_specs=placed, out_specs=out_placed, check_vma=False)
        return mapped(inputs, gate_pre, up_pre, cotangent, w_gate, w_up, w_down)

    return whole
```

```python
import functools

import jax
import jax.numpy as jnp
from jax import lax
from jax.experimental import pallas as pl
from jax.experimental.pallas import tpu as pltpu
from jax.sharding import PartitionSpec as P

LANES = 128
CHUNK = 256
LATE = 4
AHEAD = 3
VMEM_LIMIT = 56 * 2**20
F32 = jnp.float32
BF16 = jnp.bfloat16
MESH = pl.DeviceIdType.MESH
NT = (((1,), (1,)), ((), ()))


def on_device(inputs, gate_pre, up_pre, cotangent, w_gate, w_up, w_down):
    single = jnp.float32
    groups = lax.axis_size("rep")
    width = w_down.shape[1]
    own_cot = lax.dynamic_slice_in_dim(cotangent, lax.axis_index("fs") * width, width, 1)
    partial_grad = jnp.einsum("td,fd->tf", own_cot, w_down, preferred_element_type=single)
    hidden_grad = lax.psum(partial_grad.astype(jnp.bfloat16), "fs").astype(jnp.float32)
    gate = gate_pre.astype(single)
    upper = up_pre.astype(single)
    sigma = jax.nn.sigmoid(gate)
    active = gate * sigma
    hidden = (active * upper).astype(jnp.bfloat16)
    d_up = (hidden_grad * active).astype(jnp.bfloat16)
    d_gate = (hidden_grad * upper * sigma * (1.0 + gate * (1.0 - sigma))).astype(jnp.bfloat16)
    factor = float(inputs.shape[0] * groups) ** (-0.5)
    owned = width // groups
    hunits = w_gate.shape[1]
    gate_local = jnp.einsum("td,tf->df", inputs, d_gate, preferred_element_type=single) * factor
    gate_parts = lax.all_to_all(
        gate_local.reshape(owned, groups, hunits).astype(jnp.bfloat16),
        "rep",
        split_axis=1,
        concat_axis=1,
        tiled=True,
    ).astype(jnp.float32)
    grad_gate = jnp.sum(gate_parts, axis=1, keepdims=True)
    up_local = jnp.einsum("td,tf->df", inputs, d_up, preferred_element_type=single) * factor
    up_parts = lax.all_to_all(
        up_local.reshape(owned, groups, hunits).astype(jnp.bfloat16),
        "rep",
        split_axis=1,
        concat_axis=1,
        tiled=True,
    ).astype(jnp.float32)
    grad_up = jnp.sum(up_parts, axis=1, keepdims=True)
    down_local = jnp.einsum("tf,td->fd", hidden, own_cot, preferred_element_type=single) * factor
    down_parts = lax.all_to_all(
        down_local.reshape(hunits, owned, groups).astype(jnp.bfloat16),
        "rep",
        split_axis=2,
        concat_axis=2,
        tiled=True,
    ).astype(jnp.float32)
    grad_down = jnp.sum(down_parts, axis=2, keepdims=True)
    input_term = jnp.einsum("tf,df->td", d_gate, w_gate, preferred_element_type=single)
    input_term = input_term + jnp.einsum("tf,df->td", d_up, w_up, preferred_element_type=single)
    grad_input = lax.psum(input_term.astype(jnp.bfloat16), "tp")
    gate_norms, up_norms = lax.psum(
        (jnp.sum(grad_gate * grad_gate, axis=2), jnp.sum(grad_up * grad_up, axis=2)), "tp"
    )
    down_norms = lax.psum(jnp.sum(grad_down * grad_down, axis=(1, 2)), ("rep", "fs"))
    return (grad_input, grad_gate, grad_up, grad_down, gate_norms, up_norms, down_norms)


def line_kernel(
    sizes, x_hbm, gate_hbm, up_hbm, cot_hbm, wg_hbm, wu_hbm, wd_hbm,
    gi_ref, gate_out, up_out, down_out, gu_norm_ref, down_norm_ref,
    x_ref, gate_ref, up_ref, cot_ref, wg_ref, wu_ref, wd_ref,
    left, left_far, right, right_far, pg_own, pg_peer, ab, sb, bb, gi_acc, gi_own, gi_peer,
    squares, gu_own, gu_peer, dn_own, dn_peer, dn_sum,
    load_sem, sends, y_recv, a_recv, bc_recv, d_recv, r_recv, f_recv, l_recv, m_recv, gg_recv, sums_recv, dn_recv,
):
    n_fs, n_tp, factor = sizes
    y_send, a_send, b_send, c_send, r_send, f_send, l_send, m_send, gi_send, gg_send, gn_send, dn_send = (
        sends.at[k] for k in range(12)
    )
    gi_recv, gn_recv = (sums_recv.at[k] for k in range(2))
    tokens, width = x_ref.shape
    hunits = gate_ref.shape[1]
    blocks = hunits // LANES
    items = 3 * blocks
    owned = width // 4
    share = tokens // n_tp
    rep, fs, tp = lax.axis_index("rep"), lax.axis_index("fs"), lax.axis_index("tp")
    side = rep // 2
    mid, end = 1 + side, 3 * side
    far_mid, far_end = 2 - side, 3 - 3 * side
    at_end = rep == end
    partner = mid + end - rep
    fs_peer = 1 - fs
    tp_next = tp + 1 - 2 * lax.rem(tp, 2)
    tp_far = lax.rem(tp + 2, n_tp)

    first = AHEAD * LANES
    rest = hunits - first
    loads = [
        pltpu.make_async_copy(cot_hbm.at[:, pl.ds(pl.multiple_of(fs * width, LANES), width)], cot_ref, load_sem.at[0]),
        pltpu.make_async_copy(wd_hbm.at[pl.ds(0, first)], wd_ref.at[pl.ds(0, first)], load_sem.at[1]),
        pltpu.make_async_copy(gate_hbm, gate_ref, load_sem.at[2]),
        pltpu.make_async_copy(up_hbm, up_ref, load_sem.at[3]),
        pltpu.make_async_copy(x_hbm, x_ref, load_sem.at[4]),
        pltpu.make_async_copy(wg_hbm, wg_ref, load_sem.at[5]),
        pltpu.make_async_copy(wu_hbm, wu_ref, load_sem.at[6]),
        pltpu.make_async_copy(wd_hbm.at[pl.ds(first, rest)], wd_ref.at[pl.ds(first, rest)], load_sem.at[7]),
    ]

    def load(*which):
        for k in which:
            loads[k].start()

    load(4, 0, 1)

    def in_tp(step):
        return (rep, fs, lax.rem(tp + step, n_tp))

    barrier = pltpu.get_barrier_semaphore()
    greeted = [(partner, fs, tp), (rep, fs_peer, tp)] + [in_tp(s) for s in range(1, n_tp)]
    for other in greeted:
        pl.semaphore_signal(barrier, inc=1, device_id=other, device_id_type=MESH)

    @pl.when(jnp.logical_not(at_end))
    def _():
        pl.semaphore_signal(barrier, inc=1, device_id=(far_mid, fs, tp), device_id_type=MESH)

    def remote(src, dst, send, recv, other):
        return pltpu.make_async_remote_copy(
            src_ref=src, dst_ref=dst, send_sem=send, recv_sem=recv, device_id=other, device_id_type=MESH
        )

    def rows_of(slot):
        return slice(slot * owned, (slot + 1) * owned)

    def y_copy(j):
        return remote(pg_own.at[j], pg_peer.at[j], y_send, y_recv.at[j], (rep, fs_peer, tp))

    def a_copy(t, late):
        piece = ab.at[t, pl.ds(0, owned) if late else pl.ds(owned, 2 * owned)]
        k = blocks * late + t
        return remote(piece, piece, a_send, a_recv.at[k], (partner, fs, tp))

    def b_copy(kind, t):
        src = ab.at[t, pl.ds(owned, 2 * owned)] if kind == 0 else sb.at[t - blocks]
        return remote(src, bb.at[t], b_send, bc_recv.at[t], (far_mid, fs, tp))

    def last_copy(t, slot):
        rows = pl.ds(slot * owned, owned)
        recv = d_recv.at[t - items + 4] if slot else bc_recv.at[t]
        return remote(sb.at[t - blocks, rows], bb.at[t, rows], b_send, recv, (far_mid, fs, tp))

    def c_copy(t):
        return remote(
            bb.at[t, pl.ds(owned, owned)], bb.at[t, pl.ds(0, owned)], c_send, bc_recv.at[t], (partner, fs, tp)
        )

    half = tokens // n_fs
    own_half = pl.ds(pl.multiple_of(fs * half, 16), half)

    def r_copy(q):
        return remote(
            right.at[blocks + q, own_half], right_far.at[q, own_half], r_send, r_recv.at[q], (partner, fs, tp)
        )

    def f_copy(q):
        piece = right_far.at[q, own_half]
        return remote(piece, piece, f_send, f_recv.at[q], (rep, fs_peer, tp))

    piece_rows = owned // n_tp

    def piece_of(slot, owner):
        return pl.ds(pl.multiple_of(slot * owned + owner * piece_rows, 16), piece_rows)

    def l_copy(slot):
        rows = piece_of(slot, tp)
        return remote(left.at[1, rows], left_far.at[rows], l_send, l_recv.at[slot], (partner, fs, tp))

    def m_copy(slot, hop):
        piece = left_far.at[piece_of(slot, tp_far if hop == 2 else tp)]
        k = 3 * slot + hop
        return remote(piece, piece, m_send, m_recv.at[k], (rep, fs, tp_next if hop else tp_far))

    def lanes(j):
        return pl.ds(pl.multiple_of(j * LANES, LANES), LANES)

    def term(kind, first, last, t):
        rows = slice(first * owned, last * owned)
        return jnp.dot(left[kind, rows, :], right[t], preferred_element_type=F32) * factor

    def long_term(first, last, t):
        rows = slice(first * owned, last * owned)
        own = jnp.dot(left[1, rows, :], right[t], preferred_element_type=F32)
        far = jnp.dot(left_far[rows, :], right_far[t - blocks], preferred_element_type=F32)
        return (own + far) * factor

    def loop(first, last, body):
        def step(i, carry):
            body(i)
            return carry
        lax.fori_loop(first, last, step, 0)

    def spread(kind, source):
        rows = CHUNK // 4
        lane = lax.broadcasted_iota(jnp.int32, (rows, CHUNK), 1)
        place = lax.broadcasted_iota(jnp.int32, (rows, CHUNK), 0) * 4
        pick = jnp.concatenate(
            [(place + owner == lane).astype(F32).astype(BF16) for owner in (mid, far_mid, far_end, end)], axis=0
        )
        for c in range(width // CHUNK):
            picked = lax.dot_general(
                pick, source[:, c * CHUNK:(c + 1) * CHUNK], NT, preferred_element_type=F32
            ).astype(BF16)
            for slot in range(4):
                left[kind, slot * owned + c * rows:slot * owned + (c + 1) * rows, :] = picked[slot * rows:(slot + 1) * rows]

    def item(kind, j):
        return j if kind == 0 else blocks + 2 * j + kind - 1

    def hidden_of(j):
        g = gate_ref[:, lanes(j)].astype(F32)
        u = up_ref[:, lanes(j)].astype(F32)
        right[j] = (g * (1.0 / (1.0 + jnp.exp(-g))) * u).astype(BF16)

    def send_down(t):
        ab[t] = term(0, 0, 3, t).astype(BF16)
        a_copy(t, 0).start()

    def partial_of(j):
        rows = pl.ds(pl.multiple_of(j * LANES, LANES), LANES)
        pg_own[j] = lax.dot_general(cot_ref[...], wd_ref[rows, :], NT, preferred_element_type=F32).astype(BF16)

    def partial_out(j):
        partial_of(j)
        y_copy(j).start()

    def grads_of(j):
        y_copy(j).wait_recv()
        g = gate_ref[:, lanes(j)].astype(F32)
        u = up_ref[:, lanes(j)].astype(F32)
        total = pg_own[j].astype(F32) + pg_peer[j].astype(F32)
        s = 1.0 / (1.0 + jnp.exp(-g))
        t = blocks + 2 * j
        right[t] = (total * u * s * (1.0 + g * (1.0 - s))).astype(BF16)
        right[t + 1] = (total * (g * s)).astype(BF16)

    def finish(kind, j, piece):
        if kind == 0:
            dn_own[0:1, lanes(j)] = jnp.sum(piece * piece, axis=0, keepdims=True)
            down_out[pl.ds(pl.multiple_of(j * LANES, LANES), LANES), 0, :] = piece.T
        else:
            squares[kind - 1] += piece * piece
            (gate_out if kind == 1 else up_out)[:, 0, lanes(j)] = piece

    def down_on(t):
        a_copy(t, 0).wait_recv()
        rows = slice(owned, 3 * owned)
        ab[t, rows, :] = (ab[t, rows, :].astype(F32) + term(0, 1, 3, t)).astype(BF16)
        b_copy(0, t).start()

    def forward(q):
        r_copy(q).wait_recv()
        f_copy(q).start()

    def pair_on(kind, j):
        t = item(kind, j)
        f_copy(t - blocks).wait_recv()
        sb[t - blocks] = long_term(1, 3, t).astype(BF16)
        b_copy(kind, t).start()

    def settle(kind, j):
        t = item(kind, j)
        b_copy(kind, t).wait_recv()
        bb[t, owned:, :] = (bb[t, owned:, :].astype(F32) + term(min(kind, 1), 3, 4, t)).astype(BF16)
        c_copy(t).start()
        if kind:
            finish(kind, j, long_term(0, 1, t) + bb[t, :owned, :].astype(F32))

    def last_on(t):
        f_copy(t - blocks).wait_recv()
        sb[t - blocks] = long_term(1, 3, t).astype(BF16)
        last_copy(t, 1).start()

    def last_settle(t):
        last_copy(t, 1).wait_recv()
        bb[t, owned:, :] = (bb[t, owned:, :].astype(F32) + term(1, 3, 4, t)).astype(BF16)
        c_copy(t).start()

    def last_own(kind, j):
        t = item(kind, j)
        last_copy(t, 0).wait_recv()
        finish(kind, j, long_term(0, 1, t) + bb[t, :owned, :].astype(F32))

    def settle_own(j):
        a_copy(j, 1).wait_recv()
        finish(0, j, ab[j, :owned, :].astype(F32) + term(0, 0, 1, j) + bb[j, :owned, :].astype(F32))

    def last_hop(kind, j):
        t = item(kind, j)
        c_copy(t).wait_recv()
        finish(kind, j, bb[t, :owned, :].astype(F32) + term(min(kind, 1), 3, 4, t))

    def gi_term(j):
        t = blocks + 2 * j
        gi_acc[...] += lax.dot_general(right[t], wg_ref[:, lanes(j)], NT, preferred_element_type=F32) + lax.dot_general(
            right[t + 1], wu_ref[:, lanes(j)], NT, preferred_element_type=F32
        )

    def grads_and_term(j):
        grads_of(j)
        gi_term(j)

    def tokens_of(owner):
        return pl.ds(pl.multiple_of(owner * share, share), share)

    def gi_copy(step):
        other = lax.rem(tp + step, n_tp)
        return remote(
            gi_own.at[tokens_of(other)], gi_peer.at[step - 1], gi_send, gi_recv, in_tp(step)
        )

    def gg_copy(hop):
        piece = gi_ref.at[tokens_of(tp_far if hop == 2 else tp)]
        return remote(piece, piece, gg_send, gg_recv.at[hop], (rep, fs, tp_next if hop else tp_far))

    def gi_out():
        gi_own[...] = gi_acc[...].astype(BF16)
        for step in range(1, n_tp):
            gi_copy(step).start()

    here = (rep, fs_peer, tp)

    def all_in(whole, recv):
        remote(whole, whole, gi_send, recv, here).wait_recv()

    def all_out(whole, send):
        remote(whole, whole, send, gi_recv, here).wait_send()

    def gi_sum():
        all_in(gi_peer, gi_recv)
        whole = gi_own[tokens_of(tp), :].astype(F32)
        for step in range(1, n_tp):
            whole += gi_peer[step - 1].astype(F32)
        gi_ref[tokens_of(tp), :] = whole.astype(BF16)
        gg_copy(0).start()
        gg_copy(1).start()

    def gi_pass():
        gg_copy(0).wait_recv()
        gg_copy(2).start()

    def dn_copy(k):
        src = dn_sum.at[k] if k < 3 else dn_own
        place, other = ((1, (rep, fs_peer, tp)), (2, (far_mid, fs, tp)), (0, (partner, fs, tp)), (0, (partner, fs, tp)))[k]
        return remote(src, dn_peer.at[place], dn_send, dn_recv.at[place], other)

    def dn_on(k):
        dn_copy((3, 0, 1)[k]).wait_recv()
        dn_sum[k] = (dn_sum[k - 1] if k else dn_own[...]) + dn_peer[k]
        dn_copy(k).start()

    def gn_copy(step):
        return remote(gu_own, gu_peer.at[step - 1], gn_send, gn_recv, in_tp(step))

    loads[4].wait()
    load(2, 3)
    spread(1, x_ref)
    loads[0].wait()
    loads[1].wait()
    load(7)
    loop(0, 1, partial_of)

    @pl.when(at_end)
    def _():
        pl.semaphore_wait(barrier, len(greeted))

    @pl.when(jnp.logical_not(at_end))
    def _():
        pl.semaphore_wait(barrier, len(greeted) + 1)

    y_copy(0).start()

    turn = blocks // 2

    def past(j, k):
        return jnp.where(j > k, 1, 0)

    def down_from(j):
        return jnp.minimum(j + 1 + past(j, turn) + past(j, turn + 2), blocks)

    def down_to(j):
        return jnp.minimum(j + 2 + past(j, turn - 1) + past(j, turn + 1), blocks)

    def late_to(j):
        return jnp.minimum(sum(jnp.maximum(j - LATE + k, 0) for k in (1, -1, -3)), blocks)

    def sent_to(j):
        return jnp.minimum(j + AHEAD + past(j, 1), blocks)

    def grads_to(j):
        return jnp.minimum(j + AHEAD + past(j, 3), blocks)

    @pl.when(at_end)
    def _():
        l_copy(1).start()

    spread(0, cot_ref)
    loads[2].wait()
    loads[3].wait()
    load(5, 6)

    @pl.when(at_end)
    def _():
        def out(j):
            hidden_of(j)
            send_down(j)

        def pair_out(j):
            grads_of(j)
            r_copy(2 * j).start()
            r_copy(2 * j + 1).start()

        loop(0, 1, out)
        l_copy(2).start()
        loop(1, AHEAD, partial_out)
        loads[7].wait()
        loop(AHEAD, 6, partial_out)
        gi_acc[...] = jnp.zeros_like(gi_acc)

        def both_out(j):
            pair_out(j)
            loop(down_from(j), down_to(j), out)

            @pl.when(j == 1)
            def _():
                l_copy(0).start()

            loop(late_to(j - 1), late_to(j), lambda t: a_copy(t, 1).start())

        loop(0, 1, both_out)
        loop(6, blocks, partial_out)
        loop(1, blocks, both_out)
        squares[...] = jnp.zeros_like(squares)
        loads[5].wait()
        loads[6].wait()
        loop(0, blocks, gi_term)
        gi_out()

        def hops(j):
            loop(down_from(j - 2), down_to(j - 2), functools.partial(last_hop, 0))
            last_hop(1, j - 2)
            last_hop(2, j - 2)

        loop(0, 1, functools.partial(last_hop, 0))
        loop(2, blocks - 3, hops)
        gi_sum()
        loop(blocks - 3, blocks - 1, hops)
        dn_copy(3).start()
        gi_pass()
        loop(blocks - 1, blocks, hops)
        last_hop(1, blocks - 2)
        last_hop(2, blocks - 2)
        last_hop(1, blocks - 1)
        last_hop(2, blocks - 1)

    @pl.when(jnp.logical_not(at_end))
    def _():
        def spread_on(slot):
            l_copy(slot).wait_recv()
            m_copy(slot, 0).start()
            m_copy(slot, 1).start()

        def pass_on(slot):
            m_copy(slot, 0).wait_recv()
            m_copy(slot, 2).start()

        def landed(slot):
            m_copy(slot, 1).wait_recv()
            m_copy(slot, 2).wait_recv()

        def feed(j):
            forward(2 * j)
            forward(2 * j + 1)

            loop(sent_to(j - 1), sent_to(j), lambda k: y_copy(k).start())

        loop(1, 2, partial_out)
        loop(2, AHEAD, partial_of)
        loads[7].wait()
        loop(AHEAD, 8, partial_of)
        spread_on(1)
        loop(8, blocks, partial_of)
        loop(0, blocks, hidden_of)
        down_on(0)
        grads_of(0)
        spread_on(2)
        pass_on(1)
        gi_acc[...] = jnp.zeros_like(gi_acc)
        squares[...] = jnp.zeros_like(squares)
        feed(0)
        pass_on(2)
        loads[5].wait()
        loads[6].wait()
        landed(1)
        landed(2)

        def step(j):
            pair_on(1, j)
            loop(down_from(j), down_to(j), down_on)
            pair_on(2, j)

            @pl.when(j + 1 < blocks)
            def _():
                feed(j + 1)

            @pl.when(j == 0)
            def _():
                gi_term(0)
                grads_and_term(1)

            loop(grads_to(j - 1), grads_to(j), grads_and_term)

        def settles(j):
            loop(down_from(j - 2), down_to(j - 2), functools.partial(settle, 0))
            settle(1, j - 2)
            settle(2, j - 2)
            loop(late_to(j - 2), late_to(j - 1), settle_own)

        loop(0, 2, step)
        spread_on(0)
        loop(0, 1, functools.partial(settle, 0))
        pass_on(0)
        step(2)
        landed(0)

        def both(j):
            settles(j - 1)
            step(j)

        loop(3, blocks - 3, both)
        gi_out()
        loop(blocks - 3, blocks - 2, both)
        settles(blocks - 3)
        loop(items - 4, items - 2, last_on)
        feed(blocks - 1)
        gi_sum()
        settles(blocks - 2)
        loop(items - 2, items, last_on)
        loop(items - 4, items, lambda t: last_copy(t, 0).start())
        settles(blocks - 1)
        gi_pass()
        dn_on(0)
        loop(items - 4, items, last_settle)
        dn_on(1)
        for j in (blocks - 2, blocks - 1):
            last_own(1, j)
            last_own(2, j)
        dn_on(2)
        down_norm_ref[...] = dn_sum[2]

    for kind in range(2):
        gu_own[0:1, kind * owned:(kind + 1) * owned] = jnp.sum(squares[kind].T, axis=0, keepdims=True)
    for step in range(1, n_tp):
        gn_copy(step).start()

    @pl.when(at_end)
    def _():
        dn_copy(2).wait_recv()
        down_norm_ref[...] = dn_peer[0]

    gg_copy(1).wait_recv()
    gg_copy(2).wait_recv()
    all_out(gi_peer, gi_send)
    all_out(gi_ref.at[pl.ds(0, 3 * share)], gg_send)
    all_out(pg_peer, y_send)

    @pl.when(at_end)
    def _():
        all_out(left_far.at[pl.ds(0, 3 * piece_rows)], l_send)
        all_out(ab, a_send)
        all_out(dn_own, dn_send)
        all_out(right_far.at[:, own_half], r_send)

    @pl.when(jnp.logical_not(at_end))
    def _():
        all_out(left_far.at[pl.ds(0, 9 * piece_rows)], m_send)
        all_out(bb, b_send)
        all_out(dn_sum, dn_send)
        all_out(bb.at[:, pl.ds(0, owned)], c_send)
        all_out(right_far.at[:, own_half], f_send)

    all_in(gu_peer, gn_recv)
    gate_up = gu_own[...]
    for step in range(1, n_tp):
        gate_up += gu_peer[step - 1]
    gu_norm_ref[...] = gate_up
    all_out(gu_peer, gn_send)


def store_kernel(gi_ref, gate_ref, up_ref, down_ref, gu_ref, dn_ref, *rest):
    sem, line, outs = rest[-1], rest[-2], rest[:-2]
    owned = gu_ref.shape[1] // 2
    sources = (
        gate_ref, up_ref, down_ref, gi_ref, gu_ref.at[:, pl.ds(0, owned)], gu_ref.at[:, pl.ds(owned, owned)]
    )
    copies = [pltpu.make_async_copy(src, dst, sem.at[k]) for k, (src, dst) in enumerate(zip(sources, outs))]
    for copy in copies:
        copy.start()
    line[...] = dn_ref[0, :]
    for copy in copies:
        copy.wait()


def on_line(inputs, gate_pre, up_pre, cotangent, w_gate, w_up, w_down):
    n_fs, n_tp = lax.axis_size("fs"), lax.axis_size("tp")
    tokens, width = inputs.shape
    hunits = w_gate.shape[1]
    blocks = hunits // LANES
    items = 3 * blocks
    owned = width // 4
    share = tokens // n_tp
    dma = pltpu.SemaphoreType.DMA
    vmem = pltpu.VMEM
    sizes = (n_fs, n_tp, float(tokens * 4) ** (-0.5))
    shaped = jax.ShapeDtypeStruct
    gi_shape = shaped((tokens, width), BF16)
    row_shape = shaped((owned, 1, hunits), F32)
    down_shape = shaped((hunits, 1, owned), F32)
    results = pl.pallas_call(
        functools.partial(line_kernel, sizes),
        out_shape=(
            vmem((tokens, width), BF16),
            vmem((owned, 1, hunits), F32),
            vmem((owned, 1, hunits), F32),
            vmem((hunits, 1, owned), F32),
            vmem((1, 2 * owned), F32),
            vmem((1, hunits), F32),
        ),
        in_specs=[pl.BlockSpec(memory_space=pltpu.HBM)] * 7,
        out_specs=(pl.BlockSpec(memory_space=vmem),) * 6,
        scratch_shapes=[
            vmem((tokens, width), BF16),
            vmem((tokens, hunits), BF16),
            vmem((tokens, hunits), BF16),
            vmem((tokens, width), BF16),
            vmem((width, hunits), BF16),
            vmem((width, hunits), BF16),
            vmem((hunits, width), BF16),
            vmem((2, width, tokens), BF16),
            vmem((3 * owned, tokens), BF16),
            vmem((items, tokens, LANES), BF16),
            vmem((2 * blocks, tokens, LANES), BF16),
            vmem((blocks, tokens, LANES), BF16),
            vmem((blocks, tokens, LANES), BF16),
            vmem((blocks, 3 * owned, LANES), BF16),
            vmem((2 * blocks, 2 * owned, LANES), BF16),
            vmem((items, 2 * owned, LANES), BF16),
            vmem((tokens, width), F32),
            vmem((tokens, width), BF16),
            vmem((n_tp - 1, share, width), BF16),
            vmem((2, owned, LANES), F32),
            vmem((1, 2 * owned), F32),
            vmem((n_tp - 1, 1, 2 * owned), F32),
            vmem((1, hunits), F32),
            vmem((3, 1, hunits), F32),
            vmem((3, 1, hunits), F32),
            dma((8,)),
            dma((12,)),
            dma((blocks,)),
            dma((2 * blocks,)),
            dma((items,)),
            dma((4,)),
            dma((2 * blocks,)),
            dma((2 * blocks,)),
            dma((3,)),
            dma((9,)),
            dma((3,)),
            dma((2,)),
            dma((3,)),
        ],
        compiler_params=pltpu.CompilerParams(
            collective_id=0, has_side_effects=True, vmem_limit_bytes=VMEM_LIMIT
        ),
    )(inputs, gate_pre, up_pre, cotangent, w_gate, w_up, w_down)
    grad_gate, grad_up, grad_down, grad_input, gate_norms, up_norms, down_norms = pl.pallas_call(
        store_kernel,
        out_shape=(
            row_shape, row_shape, down_shape, gi_shape,
            shaped((1, owned), F32), shaped((1, owned), F32), shaped((hunits,), F32),
        ),
        in_specs=[pl.BlockSpec(memory_space=vmem)] * 6,
        out_specs=(pl.BlockSpec(memory_space=pltpu.HBM),) * 6 + (pl.BlockSpec(memory_space=vmem),),
        scratch_shapes=[dma((6,))],
        compiler_params=pltpu.CompilerParams(vmem_limit_bytes=2**23),
    )(*results)
    return (
        grad_input,
        grad_gate,
        grad_up,
        grad_down.transpose(0, 2, 1),
        gate_norms.reshape(owned, 1),
        up_norms.reshape(owned, 1),
        down_norms,
    )


def fits_line(mesh, inputs, w_gate):
    n_rep, n_fs, n_tp = (mesh.shape[axis] for axis in ("rep", "fs", "tp"))
    tokens, width = inputs.shape[0] // n_rep, inputs.shape[1] // n_fs
    return (
        n_rep == 4 and n_fs == 2 and n_tp == 4 and w_gate.shape[1] // n_tp >= 10 * LANES
        and width % (4 * LANES) == 0
        and tokens % (16 * n_tp) == 0 and tokens % LANES == 0
        and (w_gate.shape[1] // n_tp) % LANES == 0
    )


def solution(mesh):
    placed = (
        P("rep", "fs"),
        P("rep", "tp"),
        P("rep", "tp"),
        P("rep", None),
        P("fs", "tp"),
        P("fs", "tp"),
        P("tp", "fs"),
    )
    out_placed = (
        P("rep", "fs"),
        P("fs", "rep", "tp"),
        P("fs", "rep", "tp"),
        P("tp", "fs", "rep"),
        P("fs", "rep"),
        P("fs", "rep"),
        P("tp"),
    )

    def whole(inputs, gate_pre, up_pre, cotangent, w_gate, w_up, w_down):
        body = on_line if fits_line(mesh, inputs, w_gate) else on_device
        mapped = jax.shard_map(body, mesh=mesh, in_specs=placed, out_specs=out_placed, check_vma=False)
        return mapped(inputs, gate_pre, up_pre, cotangent, w_gate, w_up, w_down)

    return whole
```

```python
import functools

import jax
import jax.numpy as jnp
from jax import lax
from jax.experimental import pallas as pl
from jax.experimental.pallas import tpu as pltpu
from jax.sharding import PartitionSpec as P

LANES = 128
CHUNK = 256
LATE = 4
AHEAD = 3
VMEM_LIMIT = 56 * 2**20
F32 = jnp.float32
BF16 = jnp.bfloat16
MESH = pl.DeviceIdType.MESH
NT = (((1,), (1,)), ((), ()))


def on_device(inputs, gate_pre, up_pre, cotangent, w_gate, w_up, w_down):
    single = jnp.float32
    groups = lax.axis_size("rep")
    width = w_down.shape[1]
    own_cot = lax.dynamic_slice_in_dim(cotangent, lax.axis_index("fs") * width, width, 1)
    partial_grad = jnp.einsum("td,fd->tf", own_cot, w_down, preferred_element_type=single)
    hidden_grad = lax.psum(partial_grad.astype(jnp.bfloat16), "fs").astype(jnp.float32)
    gate = gate_pre.astype(single)
    upper = up_pre.astype(single)
    sigma = jax.nn.sigmoid(gate)
    active = gate * sigma
    hidden = (active * upper).astype(jnp.bfloat16)
    d_up = (hidden_grad * active).astype(jnp.bfloat16)
    d_gate = (hidden_grad * upper * sigma * (1.0 + gate * (1.0 - sigma))).astype(jnp.bfloat16)
    factor = float(inputs.shape[0] * groups) ** (-0.5)
    owned = width // groups
    hunits = w_gate.shape[1]
    gate_local = jnp.einsum("td,tf->df", inputs, d_gate, preferred_element_type=single) * factor
    gate_parts = lax.all_to_all(
        gate_local.reshape(owned, groups, hunits).astype(jnp.bfloat16),
        "rep",
        split_axis=1,
        concat_axis=1,
        tiled=True,
    ).astype(jnp.float32)
    grad_gate = jnp.sum(gate_parts, axis=1, keepdims=True)
    up_local = jnp.einsum("td,tf->df", inputs, d_up, preferred_element_type=single) * factor
    up_parts = lax.all_to_all(
        up_local.reshape(owned, groups, hunits).astype(jnp.bfloat16),
        "rep",
        split_axis=1,
        concat_axis=1,
        tiled=True,
    ).astype(jnp.float32)
    grad_up = jnp.sum(up_parts, axis=1, keepdims=True)
    down_local = jnp.einsum("tf,td->fd", hidden, own_cot, preferred_element_type=single) * factor
    down_parts = lax.all_to_all(
        down_local.reshape(hunits, owned, groups).astype(jnp.bfloat16),
        "rep",
        split_axis=2,
        concat_axis=2,
        tiled=True,
    ).astype(jnp.float32)
    grad_down = jnp.sum(down_parts, axis=2, keepdims=True)
    input_term = jnp.einsum("tf,df->td", d_gate, w_gate, preferred_element_type=single)
    input_term = input_term + jnp.einsum("tf,df->td", d_up, w_up, preferred_element_type=single)
    grad_input = lax.psum(input_term.astype(jnp.bfloat16), "tp")
    gate_norms, up_norms = lax.psum(
        (jnp.sum(grad_gate * grad_gate, axis=2), jnp.sum(grad_up * grad_up, axis=2)), "tp"
    )
    down_norms = lax.psum(jnp.sum(grad_down * grad_down, axis=(1, 2)), ("rep", "fs"))
    return (grad_input, grad_gate, grad_up, grad_down, gate_norms, up_norms, down_norms)


def line_kernel(
    sizes, x_hbm, gate_hbm, up_hbm, cot_hbm, wg_hbm, wu_hbm, wd_hbm,
    gi_ref, gate_out, up_out, down_out, gu_norm_ref, down_norm_ref,
    x_ref, gate_ref, up_ref, cot_ref, wg_ref, wu_ref, wd_ref,
    left, left_far, right, right_far, pg_own, pg_peer, ab, sb, bb, gi_acc, gi_own, gi_peer,
    squares, gu_own, gu_peer, dn_own, dn_peer, dn_sum,
    load_sem, sends, y_recv, a_recv, bc_recv, d_recv, r_recv, f_recv, l_recv, m_recv, gg_recv, sums_recv, dn_recv,
):
    n_fs, n_tp, factor = sizes
    y_send, a_send, b_send, c_send, r_send, f_send, l_send, m_send, gi_send, gg_send, gn_send, dn_send = (
        sends.at[k] for k in range(12)
    )
    gi_recv, gn_recv = (sums_recv.at[k] for k in range(2))
    tokens, width = x_ref.shape
    hunits = gate_ref.shape[1]
    blocks = hunits // LANES
    items = 3 * blocks
    owned = width // 4
    share = tokens // n_tp
    rep, fs, tp = lax.axis_index("rep"), lax.axis_index("fs"), lax.axis_index("tp")
    side = rep // 2
    mid, end = 1 + side, 3 * side
    far_mid, far_end = 2 - side, 3 - 3 * side
    at_end = rep == end
    partner = mid + end - rep
    fs_peer = 1 - fs
    tp_next = tp + 1 - 2 * lax.rem(tp, 2)
    tp_far = lax.rem(tp + 2, n_tp)

    first = AHEAD * LANES
    rest = hunits - first
    loads = [
        pltpu.make_async_copy(cot_hbm.at[:, pl.ds(pl.multiple_of(fs * width, LANES), width)], cot_ref, load_sem.at[0]),
        pltpu.make_async_copy(wd_hbm.at[pl.ds(0, first)], wd_ref.at[pl.ds(0, first)], load_sem.at[1]),
        pltpu.make_async_copy(gate_hbm, gate_ref, load_sem.at[2]),
        pltpu.make_async_copy(up_hbm, up_ref, load_sem.at[3]),
        pltpu.make_async_copy(x_hbm, x_ref, load_sem.at[4]),
        pltpu.make_async_copy(wg_hbm, wg_ref, load_sem.at[5]),
        pltpu.make_async_copy(wu_hbm, wu_ref, load_sem.at[6]),
        pltpu.make_async_copy(wd_hbm.at[pl.ds(first, rest)], wd_ref.at[pl.ds(first, rest)], load_sem.at[7]),
    ]

    def load(*which):
        for k in which:
            loads[k].start()

    load(4, 0, 1)

    def in_tp(step):
        return (rep, fs, lax.rem(tp + step, n_tp))

    barrier = pltpu.get_barrier_semaphore()
    greeted = [(partner, fs, tp), (rep, fs_peer, tp)] + [in_tp(s) for s in range(1, n_tp)]
    for other in greeted:
        pl.semaphore_signal(barrier, inc=1, device_id=other, device_id_type=MESH)

    @pl.when(jnp.logical_not(at_end))
    def _():
        pl.semaphore_signal(barrier, inc=1, device_id=(far_mid, fs, tp), device_id_type=MESH)

    def remote(src, dst, send, recv, other):
        return pltpu.make_async_remote_copy(
            src_ref=src, dst_ref=dst, send_sem=send, recv_sem=recv, device_id=other, device_id_type=MESH
        )

    def rows_of(slot):
        return slice(slot * owned, (slot + 1) * owned)

    def y_copy(j):
        return remote(pg_own.at[j], pg_peer.at[j], y_send, y_recv.at[j], (rep, fs_peer, tp))

    def a_copy(t, late):
        piece = ab.at[t, pl.ds(0, owned) if late else pl.ds(owned, 2 * owned)]
        k = blocks * late + t
        return remote(piece, piece, a_send, a_recv.at[k], (partner, fs, tp))

    def b_copy(kind, t):
        src = ab.at[t, pl.ds(owned, 2 * owned)] if kind == 0 else sb.at[t - blocks]
        return remote(src, bb.at[t], b_send, bc_recv.at[t], (far_mid, fs, tp))

    def last_copy(t, slot):
        rows = pl.ds(slot * owned, owned)
        recv = d_recv.at[t - items + 4] if slot else bc_recv.at[t]
        return remote(sb.at[t - blocks, rows], bb.at[t, rows], b_send, recv, (far_mid, fs, tp))

    def c_copy(t):
        return remote(
            bb.at[t, pl.ds(owned, owned)], bb.at[t, pl.ds(0, owned)], c_send, bc_recv.at[t], (partner, fs, tp)
        )

    half = tokens // n_fs
    own_half = pl.ds(pl.multiple_of(fs * half, 16), half)

    peer_half = pl.ds(pl.multiple_of(fs_peer * half, 16), half)

    def y_half(part):
        rows = own_half if part else peer_half
        return remote(
            pg_own.at[0, rows], pg_peer.at[0, rows], y_send, y_recv.at[blocks * part], (rep, fs_peer, tp)
        )

    def quarter_of(part):
        return pl.ds(pl.multiple_of(fs * half + part * (half // 2), 16), half // 2)

    def r_first(part):
        rows = quarter_of(part)
        return remote(
            right.at[blocks, rows], right_far.at[0, rows], r_send, r_recv.at[2 * blocks * part], (partner, fs, tp)
        )

    def f_first(part):
        piece = right_far.at[0, quarter_of(part)]
        return remote(piece, piece, f_send, f_recv.at[0], (rep, fs_peer, tp))

    def r_copy(q):
        return remote(
            right.at[blocks + q, own_half], right_far.at[q, own_half], r_send, r_recv.at[q], (partner, fs, tp)
        )

    def f_copy(q):
        piece = right_far.at[q, own_half]
        return remote(piece, piece, f_send, f_recv.at[q], (rep, fs_peer, tp))

    piece_rows = owned // n_tp

    def piece_of(slot, owner):
        return pl.ds(pl.multiple_of(slot * owned + owner * piece_rows, 16), piece_rows)

    def l_copy(slot):
        rows = piece_of(slot, tp)
        return remote(left.at[1, rows], left_far.at[rows], l_send, l_recv.at[slot], (partner, fs, tp))

    def m_copy(slot, hop):
        piece = left_far.at[piece_of(slot, tp_far if hop == 2 else tp)]
        k = 3 * slot + hop
        return remote(piece, piece, m_send, m_recv.at[k], (rep, fs, tp_next if hop else tp_far))

    def lanes(j):
        return pl.ds(pl.multiple_of(j * LANES, LANES), LANES)

    def term(kind, first, last, t):
        rows = slice(first * owned, last * owned)
        return jnp.dot(left[kind, rows, :], right[t], preferred_element_type=F32) * factor

    def long_term(first, last, t):
        rows = slice(first * owned, last * owned)
        own = jnp.dot(left[1, rows, :], right[t], preferred_element_type=F32)
        far = jnp.dot(left_far[rows, :], right_far[t - blocks], preferred_element_type=F32)
        return (own + far) * factor

    def loop(first, last, body):
        def step(i, carry):
            body(i)
            return carry
        lax.fori_loop(first, last, step, 0)

    def spread(kind, source):
        rows = CHUNK // 4
        lane = lax.broadcasted_iota(jnp.int32, (rows, CHUNK), 1)
        place = lax.broadcasted_iota(jnp.int32, (rows, CHUNK), 0) * 4
        pick = jnp.concatenate(
            [(place + owner == lane).astype(F32).astype(BF16) for owner in (mid, far_mid, far_end, end)], axis=0
        )
        for c in range(width // CHUNK):
            picked = lax.dot_general(
                pick, source[:, c * CHUNK:(c + 1) * CHUNK], NT, preferred_element_type=F32
            ).astype(BF16)
            for slot in range(4):
                left[kind, slot * owned + c * rows:slot * owned + (c + 1) * rows, :] = picked[slot * rows:(slot + 1) * rows]

    def item(kind, j):
        return j if kind == 0 else blocks + 2 * j + kind - 1

    def hidden_of(j):
        g = gate_ref[:, lanes(j)].astype(F32)
        u = up_ref[:, lanes(j)].astype(F32)
        right[j] = (g * (1.0 / (1.0 + jnp.exp(-g))) * u).astype(BF16)

    def send_down(t):
        ab[t] = term(0, 0, 3, t).astype(BF16)
        a_copy(t, 0).start()

    def partial_of(j):
        rows = pl.ds(pl.multiple_of(j * LANES, LANES), LANES)
        pg_own[j] = lax.dot_general(cot_ref[...], wd_ref[rows, :], NT, preferred_element_type=F32).astype(BF16)

    def partial_out(j):
        partial_of(j)
        y_copy(j).start()

    def grads_rows(j, rows):
        g = gate_ref[rows, lanes(j)].astype(F32)
        u = up_ref[rows, lanes(j)].astype(F32)
        total = pg_own[j, rows, :].astype(F32) + pg_peer[j, rows, :].astype(F32)
        s = 1.0 / (1.0 + jnp.exp(-g))
        t = blocks + 2 * j
        right[t, rows, :] = (total * u * s * (1.0 + g * (1.0 - s))).astype(BF16)
        right[t + 1, rows, :] = (total * (g * s)).astype(BF16)

    def grads_of(j):
        y_copy(j).wait_recv()
        grads_rows(j, slice(0, tokens))

    def finish(kind, j, piece):
        if kind == 0:
            dn_own[0:1, lanes(j)] = jnp.sum(piece * piece, axis=0, keepdims=True)
            down_out[pl.ds(pl.multiple_of(j * LANES, LANES), LANES), 0, :] = piece.T
        else:
            squares[kind - 1] += piece * piece
            (gate_out if kind == 1 else up_out)[:, 0, lanes(j)] = piece

    def down_on(t):
        a_copy(t, 0).wait_recv()
        rows = slice(owned, 3 * owned)
        ab[t, rows, :] = (ab[t, rows, :].astype(F32) + term(0, 1, 3, t)).astype(BF16)
        b_copy(0, t).start()

    def forward(q):
        r_copy(q).wait_recv()
        f_copy(q).start()

    def pair_on(kind, j):
        t = item(kind, j)
        f_copy(t - blocks).wait_recv()
        sb[t - blocks] = long_term(1, 3, t).astype(BF16)
        b_copy(kind, t).start()

    def settle(kind, j):
        t = item(kind, j)
        b_copy(kind, t).wait_recv()
        bb[t, owned:, :] = (bb[t, owned:, :].astype(F32) + term(min(kind, 1), 3, 4, t)).astype(BF16)
        c_copy(t).start()
        if kind:
            finish(kind, j, long_term(0, 1, t) + bb[t, :owned, :].astype(F32))

    def last_on(t):
        f_copy(t - blocks).wait_recv()
        sb[t - blocks] = long_term(1, 3, t).astype(BF16)
        last_copy(t, 1).start()

    def last_settle(t):
        last_copy(t, 1).wait_recv()
        bb[t, owned:, :] = (bb[t, owned:, :].astype(F32) + term(1, 3, 4, t)).astype(BF16)
        c_copy(t).start()

    def last_own(kind, j):
        t = item(kind, j)
        last_copy(t, 0).wait_recv()
        finish(kind, j, long_term(0, 1, t) + bb[t, :owned, :].astype(F32))

    def settle_own(j):
        a_copy(j, 1).wait_recv()
        finish(0, j, ab[j, :owned, :].astype(F32) + term(0, 0, 1, j) + bb[j, :owned, :].astype(F32))

    def last_hop(kind, j):
        t = item(kind, j)
        c_copy(t).wait_recv()
        finish(kind, j, bb[t, :owned, :].astype(F32) + term(min(kind, 1), 3, 4, t))

    def gi_term(j):
        t = blocks + 2 * j
        gi_acc[...] += lax.dot_general(right[t], wg_ref[:, lanes(j)], NT, preferred_element_type=F32) + lax.dot_general(
            right[t + 1], wu_ref[:, lanes(j)], NT, preferred_element_type=F32
        )

    def grads_and_term(j):
        grads_of(j)
        gi_term(j)

    def tokens_of(owner):
        return pl.ds(pl.multiple_of(owner * share, share), share)

    def gi_copy(step):
        other = lax.rem(tp + step, n_tp)
        return remote(
            gi_own.at[tokens_of(other)], gi_peer.at[step - 1], gi_send, gi_recv, in_tp(step)
        )

    def gg_copy(hop):
        piece = gi_ref.at[tokens_of(tp_far if hop == 2 else tp)]
        return remote(piece, piece, gg_send, gg_recv.at[hop], (rep, fs, tp_next if hop else tp_far))

    def gi_out():
        gi_own[...] = gi_acc[...].astype(BF16)
        for step in range(1, n_tp):
            gi_copy(step).start()

    here = (rep, fs_peer, tp)

    def all_in(whole, recv):
        remote(whole, whole, gi_send, recv, here).wait_recv()

    def all_out(whole, send):
        remote(whole, whole, send, gi_recv, here).wait_send()

    def gi_sum():
        all_in(gi_peer, gi_recv)
        whole = gi_own[tokens_of(tp), :].astype(F32)
        for step in range(1, n_tp):
            whole += gi_peer[step - 1].astype(F32)
        gi_ref[tokens_of(tp), :] = whole.astype(BF16)
        gg_copy(0).start()
        gg_copy(1).start()

    def gi_pass():
        gg_copy(0).wait_recv()
        gg_copy(2).start()

    def dn_copy(k):
        src = dn_sum.at[k] if k < 3 else dn_own
        place, other = ((1, (rep, fs_peer, tp)), (2, (far_mid, fs, tp)), (0, (partner, fs, tp)), (0, (partner, fs, tp)))[k]
        return remote(src, dn_peer.at[place], dn_send, dn_recv.at[place], other)

    def dn_on(k):
        dn_copy((3, 0, 1)[k]).wait_recv()
        dn_sum[k] = (dn_sum[k - 1] if k else dn_own[...]) + dn_peer[k]
        dn_copy(k).start()

    def gn_copy(step):
        return remote(gu_own, gu_peer.at[step - 1], gn_send, gn_recv, in_tp(step))

    loads[4].wait()
    load(2, 3)
    spread(1, x_ref)

    @pl.when(at_end)
    def _():
        pl.semaphore_wait(barrier, len(greeted))
        l_copy(1).start()
        l_copy(2).start()

    @pl.when(jnp.logical_not(at_end))
    def _():
        pl.semaphore_wait(barrier, len(greeted) + 1)

    loads[0].wait()
    loads[1].wait()
    load(7)
    loop(0, 1, partial_of)

    @pl.when(at_end)
    def _():
        y_half(0).start()
        y_half(1).start()

    @pl.when(jnp.logical_not(at_end))
    def _():
        y_copy(0).start()

    turn = blocks // 2

    def past(j, k):
        return jnp.where(j > k, 1, 0)

    def down_from(j):
        return jnp.minimum(j + 1 + past(j, turn) + past(j, turn + 2), blocks)

    def down_to(j):
        return jnp.minimum(j + 2 + past(j, turn - 1) + past(j, turn + 1), blocks)

    def late_to(j):
        return jnp.minimum(sum(jnp.maximum(j - LATE + k, 0) for k in (1, -1, -3)), blocks)

    def sent_to(j):
        return jnp.minimum(j + AHEAD + past(j, 1), blocks)

    def grads_to(j):
        return jnp.minimum(j + AHEAD + past(j, 3), blocks)

    spread(0, cot_ref)
    loads[2].wait()
    loads[3].wait()
    load(5, 6)

    @pl.when(at_end)
    def _():
        def out(j):
            hidden_of(j)
            send_down(j)

        def pair_out(j):
            grads_of(j)
            r_copy(2 * j).start()
            r_copy(2 * j + 1).start()

        loop(0, 1, out)
        loop(1, AHEAD, partial_out)
        loads[7].wait()
        loop(AHEAD, 6, partial_out)
        gi_acc[...] = jnp.zeros_like(gi_acc)

        def both_out(j):
            pair_out(j)
            loop(down_from(j), down_to(j), out)

            @pl.when(j == 1)
            def _():
                l_copy(0).start()

            loop(late_to(j - 1), late_to(j), lambda t: a_copy(t, 1).start())

        y_half(0).wait_recv()
        grads_rows(0, own_half)
        r_first(0).start()
        r_first(1).start()
        r_copy(1).start()
        out(1)
        y_half(1).wait_recv()
        grads_rows(0, peer_half)
        loop(6, blocks, partial_out)
        loop(1, blocks, both_out)
        squares[...] = jnp.zeros_like(squares)
        loads[5].wait()
        loads[6].wait()
        loop(0, blocks, gi_term)
        gi_out()

        def hops(j):
            loop(down_from(j - 2), down_to(j - 2), functools.partial(last_hop, 0))
            last_hop(1, j - 2)
            last_hop(2, j - 2)

        loop(0, 1, functools.partial(last_hop, 0))
        loop(2, blocks - 3, hops)
        gi_sum()
        loop(blocks - 3, blocks - 1, hops)
        dn_copy(3).start()
        gi_pass()
        loop(blocks - 1, blocks, hops)
        last_hop(1, blocks - 2)
        last_hop(2, blocks - 2)
        last_hop(1, blocks - 1)
        last_hop(2, blocks - 1)

    @pl.when(jnp.logical_not(at_end))
    def _():
        def spread_on(slot):
            l_copy(slot).wait_recv()
            m_copy(slot, 0).start()
            m_copy(slot, 1).start()

        def pass_on(slot):
            m_copy(slot, 0).wait_recv()
            m_copy(slot, 2).start()

        def landed(slot):
            m_copy(slot, 1).wait_recv()
            m_copy(slot, 2).wait_recv()

        def feed(j):
            forward(2 * j)
            forward(2 * j + 1)

            loop(sent_to(j - 1), sent_to(j), lambda k: y_copy(k).start())

        loop(1, 2, partial_out)
        loop(2, AHEAD, partial_of)
        loads[7].wait()
        loop(AHEAD, 8, partial_of)
        spread_on(1)
        loop(8, blocks, partial_of)
        loop(0, blocks, hidden_of)
        down_on(0)
        grads_of(0)
        spread_on(2)
        pass_on(1)
        gi_acc[...] = jnp.zeros_like(gi_acc)
        squares[...] = jnp.zeros_like(squares)
        for part in range(2):
            r_first(part).wait_recv()
            f_first(part).start()
        forward(1)
        loop(2, sent_to(0), lambda k: y_copy(k).start())
        pass_on(2)
        loads[5].wait()
        loads[6].wait()
        landed(1)
        landed(2)

        def step(j):
            pair_on(1, j)
            loop(down_from(j), down_to(j), down_on)
            pair_on(2, j)

            @pl.when(j + 1 < blocks)
            def _():
                feed(j + 1)

            @pl.when(j == 0)
            def _():
                gi_term(0)
                grads_and_term(1)

            loop(grads_to(j - 1), grads_to(j), grads_and_term)

        def settles(j):
            loop(down_from(j - 2), down_to(j - 2), functools.partial(settle, 0))
            settle(1, j - 2)
            settle(2, j - 2)
            loop(late_to(j - 2), late_to(j - 1), settle_own)

        loop(0, 2, step)
        spread_on(0)
        loop(0, 1, functools.partial(settle, 0))
        pass_on(0)
        step(2)
        landed(0)

        def both(j):
            settles(j - 1)
            step(j)

        loop(3, blocks - 3, both)
        gi_out()
        loop(blocks - 3, blocks - 2, both)
        settles(blocks - 3)
        loop(items - 4, items - 2, last_on)
        feed(blocks - 1)
        gi_sum()
        settles(blocks - 2)
        loop(items - 2, items, last_on)
        loop(items - 4, items, lambda t: last_copy(t, 0).start())
        settles(blocks - 1)
        loop(items - 4, items, last_settle)
        gi_pass()
        dn_on(0)

        def owns(j):
            last_own(1, j)
            last_own(2, j)

        loop(blocks - 2, blocks - 1, owns)
        dn_on(1)
        loop(blocks - 1, blocks, owns)
        dn_on(2)
        down_norm_ref[...] = dn_sum[2]

    for kind in range(2):
        gu_own[0:1, kind * owned:(kind + 1) * owned] = jnp.sum(squares[kind].T, axis=0, keepdims=True)
    for step in range(1, n_tp):
        gn_copy(step).start()

    @pl.when(at_end)
    def _():
        dn_copy(2).wait_recv()
        down_norm_ref[...] = dn_peer[0]

    gg_copy(1).wait_recv()
    gg_copy(2).wait_recv()
    all_out(gi_peer, gi_send)
    all_out(gi_ref.at[pl.ds(0, 3 * share)], gg_send)
    all_out(pg_peer, y_send)

    @pl.when(at_end)
    def _():
        all_out(left_far.at[pl.ds(0, 3 * piece_rows)], l_send)
        all_out(ab, a_send)
        all_out(dn_own, dn_send)
        all_out(right_far.at[:, own_half], r_send)

    @pl.when(jnp.logical_not(at_end))
    def _():
        all_out(left_far.at[pl.ds(0, 9 * piece_rows)], m_send)
        all_out(bb, b_send)
        all_out(dn_sum, dn_send)
        all_out(bb.at[:, pl.ds(0, owned)], c_send)
        all_out(right_far.at[:, own_half], f_send)

    all_in(gu_peer, gn_recv)
    gate_up = gu_own[...]
    for step in range(1, n_tp):
        gate_up += gu_peer[step - 1]
    gu_norm_ref[...] = gate_up
    all_out(gu_peer, gn_send)


def store_kernel(gi_ref, gate_ref, up_ref, down_ref, gu_ref, dn_ref, *rest):
    sem, line, outs = rest[-1], rest[-2], rest[:-2]
    owned = gu_ref.shape[1] // 2
    sources = (
        gate_ref, up_ref, down_ref, gi_ref, gu_ref.at[:, pl.ds(0, owned)], gu_ref.at[:, pl.ds(owned, owned)]
    )
    copies = [pltpu.make_async_copy(src, dst, sem.at[k]) for k, (src, dst) in enumerate(zip(sources, outs))]
    for copy in copies:
        copy.start()
    line[...] = dn_ref[0, :]
    for copy in copies:
        copy.wait()


def on_line(inputs, gate_pre, up_pre, cotangent, w_gate, w_up, w_down):
    n_fs, n_tp = lax.axis_size("fs"), lax.axis_size("tp")
    tokens, width = inputs.shape
    hunits = w_gate.shape[1]
    blocks = hunits // LANES
    items = 3 * blocks
    owned = width // 4
    share = tokens // n_tp
    dma = pltpu.SemaphoreType.DMA
    vmem = pltpu.VMEM
    sizes = (n_fs, n_tp, float(tokens * 4) ** (-0.5))
    shaped = jax.ShapeDtypeStruct
    gi_shape = shaped((tokens, width), BF16)
    row_shape = shaped((owned, 1, hunits), F32)
    down_shape = shaped((hunits, 1, owned), F32)
    results = pl.pallas_call(
        functools.partial(line_kernel, sizes),
        out_shape=(
            vmem((tokens, width), BF16),
            vmem((owned, 1, hunits), F32),
            vmem((owned, 1, hunits), F32),
            vmem((hunits, 1, owned), F32),
            vmem((1, 2 * owned), F32),
            vmem((1, hunits), F32),
        ),
        in_specs=[pl.BlockSpec(memory_space=pltpu.HBM)] * 7,
        out_specs=(pl.BlockSpec(memory_space=vmem),) * 6,
        scratch_shapes=[
            vmem((tokens, width), BF16),
            vmem((tokens, hunits), BF16),
            vmem((tokens, hunits), BF16),
            vmem((tokens, width), BF16),
            vmem((width, hunits), BF16),
            vmem((width, hunits), BF16),
            vmem((hunits, width), BF16),
            vmem((2, width, tokens), BF16),
            vmem((3 * owned, tokens), BF16),
            vmem((items, tokens, LANES), BF16),
            vmem((2 * blocks, tokens, LANES), BF16),
            vmem((blocks, tokens, LANES), BF16),
            vmem((blocks, tokens, LANES), BF16),
            vmem((blocks, 3 * owned, LANES), BF16),
            vmem((2 * blocks, 2 * owned, LANES), BF16),
            vmem((items, 2 * owned, LANES), BF16),
            vmem((tokens, width), F32),
            vmem((tokens, width), BF16),
            vmem((n_tp - 1, share, width), BF16),
            vmem((2, owned, LANES), F32),
            vmem((1, 2 * owned), F32),
            vmem((n_tp - 1, 1, 2 * owned), F32),
            vmem((1, hunits), F32),
            vmem((3, 1, hunits), F32),
            vmem((3, 1, hunits), F32),
            dma((8,)),
            dma((12,)),
            dma((blocks + 1,)),
            dma((2 * blocks,)),
            dma((items,)),
            dma((4,)),
            dma((2 * blocks + 1,)),
            dma((2 * blocks,)),
            dma((3,)),
            dma((9,)),
            dma((3,)),
            dma((2,)),
            dma((3,)),
        ],
        compiler_params=pltpu.CompilerParams(
            collective_id=0, has_side_effects=True, vmem_limit_bytes=VMEM_LIMIT
        ),
    )(inputs, gate_pre, up_pre, cotangent, w_gate, w_up, w_down)
    grad_gate, grad_up, grad_down, grad_input, gate_norms, up_norms, down_norms = pl.pallas_call(
        store_kernel,
        out_shape=(
            row_shape, row_shape, down_shape, gi_shape,
            shaped((1, owned), F32), shaped((1, owned), F32), shaped((hunits,), F32),
        ),
        in_specs=[pl.BlockSpec(memory_space=vmem)] * 6,
        out_specs=(pl.BlockSpec(memory_space=pltpu.HBM),) * 6 + (pl.BlockSpec(memory_space=vmem),),
        scratch_shapes=[dma((6,))],
        compiler_params=pltpu.CompilerParams(vmem_limit_bytes=2**23),
    )(*results)
    return (
        grad_input,
        grad_gate,
        grad_up,
        grad_down.transpose(0, 2, 1),
        gate_norms.reshape(owned, 1),
        up_norms.reshape(owned, 1),
        down_norms,
    )


def fits_line(mesh, inputs, w_gate):
    n_rep, n_fs, n_tp = (mesh.shape[axis] for axis in ("rep", "fs", "tp"))
    tokens, width = inputs.shape[0] // n_rep, inputs.shape[1] // n_fs
    return (
        n_rep == 4 and n_fs == 2 and n_tp == 4 and w_gate.shape[1] // n_tp >= 10 * LANES
        and width % (4 * LANES) == 0
        and tokens % (64 * n_fs) == 0 and tokens % LANES == 0
        and (w_gate.shape[1] // n_tp) % LANES == 0
    )


def solution(mesh):
    placed = (
        P("rep", "fs"),
        P("rep", "tp"),
        P("rep", "tp"),
        P("rep", None),
        P("fs", "tp"),
        P("fs", "tp"),
        P("tp", "fs"),
    )
    out_placed = (
        P("rep", "fs"),
        P("fs", "rep", "tp"),
        P("fs", "rep", "tp"),
        P("tp", "fs", "rep"),
        P("fs", "rep"),
        P("fs", "rep"),
        P("tp"),
    )

    def whole(inputs, gate_pre, up_pre, cotangent, w_gate, w_up, w_down):
        body = on_line if fits_line(mesh, inputs, w_gate) else on_device
        mapped = jax.shard_map(body, mesh=mesh, in_specs=placed, out_specs=out_placed, check_vma=False)
        return mapped(inputs, gate_pre, up_pre, cotangent, w_gate, w_up, w_down)

    return whole
```

```python
import functools

import jax
import jax.numpy as jnp
from jax import lax
from jax.experimental import pallas as pl
from jax.experimental.pallas import tpu as pltpu
from jax.sharding import PartitionSpec as P

LANES = 128
CHUNK = 256
LATE = 6
AHEAD = 3
VMEM_LIMIT = 56 * 2**20
F32 = jnp.float32
BF16 = jnp.bfloat16
MESH = pl.DeviceIdType.MESH
NT = (((1,), (1,)), ((), ()))


def on_device(inputs, gate_pre, up_pre, cotangent, w_gate, w_up, w_down):
    single = jnp.float32
    groups = lax.axis_size("rep")
    width = w_down.shape[1]
    own_cot = lax.dynamic_slice_in_dim(cotangent, lax.axis_index("fs") * width, width, 1)
    partial_grad = jnp.einsum("td,fd->tf", own_cot, w_down, preferred_element_type=single)
    hidden_grad = lax.psum(partial_grad.astype(jnp.bfloat16), "fs").astype(jnp.float32)
    gate = gate_pre.astype(single)
    upper = up_pre.astype(single)
    sigma = jax.nn.sigmoid(gate)
    active = gate * sigma
    hidden = (active * upper).astype(jnp.bfloat16)
    d_up = (hidden_grad * active).astype(jnp.bfloat16)
    d_gate = (hidden_grad * upper * sigma * (1.0 + gate * (1.0 - sigma))).astype(jnp.bfloat16)
    factor = float(inputs.shape[0] * groups) ** (-0.5)
    owned = width // groups
    hunits = w_gate.shape[1]
    gate_local = jnp.einsum("td,tf->df", inputs, d_gate, preferred_element_type=single) * factor
    gate_parts = lax.all_to_all(
        gate_local.reshape(owned, groups, hunits).astype(jnp.bfloat16),
        "rep",
        split_axis=1,
        concat_axis=1,
        tiled=True,
    ).astype(jnp.float32)
    grad_gate = jnp.sum(gate_parts, axis=1, keepdims=True)
    up_local = jnp.einsum("td,tf->df", inputs, d_up, preferred_element_type=single) * factor
    up_parts = lax.all_to_all(
        up_local.reshape(owned, groups, hunits).astype(jnp.bfloat16),
        "rep",
        split_axis=1,
        concat_axis=1,
        tiled=True,
    ).astype(jnp.float32)
    grad_up = jnp.sum(up_parts, axis=1, keepdims=True)
    down_local = jnp.einsum("tf,td->fd", hidden, own_cot, preferred_element_type=single) * factor
    down_parts = lax.all_to_all(
        down_local.reshape(hunits, owned, groups).astype(jnp.bfloat16),
        "rep",
        split_axis=2,
        concat_axis=2,
        tiled=True,
    ).astype(jnp.float32)
    grad_down = jnp.sum(down_parts, axis=2, keepdims=True)
    input_term = jnp.einsum("tf,df->td", d_gate, w_gate, preferred_element_type=single)
    input_term = input_term + jnp.einsum("tf,df->td", d_up, w_up, preferred_element_type=single)
    grad_input = lax.psum(input_term.astype(jnp.bfloat16), "tp")
    gate_norms, up_norms = lax.psum(
        (jnp.sum(grad_gate * grad_gate, axis=2), jnp.sum(grad_up * grad_up, axis=2)), "tp"
    )
    down_norms = lax.psum(jnp.sum(grad_down * grad_down, axis=(1, 2)), ("rep", "fs"))
    return (grad_input, grad_gate, grad_up, grad_down, gate_norms, up_norms, down_norms)


def line_kernel(
    sizes, x_hbm, gate_hbm, up_hbm, cot_hbm, wg_hbm, wu_hbm, wd_hbm,
    gi_ref, gate_out, up_out, down_out, gu_norm_ref, down_norm_ref,
    x_ref, gate_ref, up_ref, cot_ref, wg_ref, wu_ref, wd_ref,
    left, left_far, right, right_far, pg_own, pg_peer, ab, sb, bb, gi_acc, gi_own, gi_peer,
    squares, gu_own, gu_peer, dn_own, dn_peer, dn_sum,
    load_sem, sends, y_recv, a_recv, bc_recv, d_recv, r_recv, f_recv, l_recv, m_recv, gg_recv, sums_recv, dn_recv,
):
    n_fs, n_tp, factor = sizes
    y_send, a_send, b_send, c_send, r_send, f_send, l_send, m_send, gi_send, gg_send, gn_send, dn_send = (
        sends.at[k] for k in range(12)
    )
    gi_recv, gn_recv = (sums_recv.at[k] for k in range(2))
    tokens, width = x_ref.shape
    hunits = gate_ref.shape[1]
    blocks = hunits // LANES
    items = 3 * blocks
    owned = width // 4
    share = tokens // n_tp
    rep, fs, tp = lax.axis_index("rep"), lax.axis_index("fs"), lax.axis_index("tp")
    side = rep // 2
    mid, end = 1 + side, 3 * side
    far_mid, far_end = 2 - side, 3 - 3 * side
    at_end = rep == end
    partner = mid + end - rep
    fs_peer = 1 - fs
    tp_next = tp + 1 - 2 * lax.rem(tp, 2)
    tp_far = lax.rem(tp + 2, n_tp)

    first = AHEAD * LANES
    rest = hunits - first
    loads = [
        pltpu.make_async_copy(cot_hbm.at[:, pl.ds(pl.multiple_of(fs * width, LANES), width)], cot_ref, load_sem.at[0]),
        pltpu.make_async_copy(wd_hbm.at[pl.ds(0, first)], wd_ref.at[pl.ds(0, first)], load_sem.at[1]),
        pltpu.make_async_copy(gate_hbm, gate_ref, load_sem.at[2]),
        pltpu.make_async_copy(up_hbm, up_ref, load_sem.at[3]),
        pltpu.make_async_copy(x_hbm, x_ref, load_sem.at[4]),
        pltpu.make_async_copy(wg_hbm, wg_ref, load_sem.at[5]),
        pltpu.make_async_copy(wu_hbm, wu_ref, load_sem.at[6]),
        pltpu.make_async_copy(wd_hbm.at[pl.ds(first, rest)], wd_ref.at[pl.ds(first, rest)], load_sem.at[7]),
    ]

    def load(*which):
        for k in which:
            loads[k].start()

    load(4, 0, 1)

    def in_tp(step):
        return (rep, fs, lax.rem(tp + step, n_tp))

    barrier = pltpu.get_barrier_semaphore()
    greeted = [(partner, fs, tp), (rep, fs_peer, tp)] + [in_tp(s) for s in range(1, n_tp)]
    for other in greeted:
        pl.semaphore_signal(barrier, inc=1, device_id=other, device_id_type=MESH)

    @pl.when(jnp.logical_not(at_end))
    def _():
        pl.semaphore_signal(barrier, inc=1, device_id=(far_mid, fs, tp), device_id_type=MESH)

    def remote(src, dst, send, recv, other):
        return pltpu.make_async_remote_copy(
            src_ref=src, dst_ref=dst, send_sem=send, recv_sem=recv, device_id=other, device_id_type=MESH
        )

    def rows_of(slot):
        return slice(slot * owned, (slot + 1) * owned)

    def y_copy(j):
        return remote(pg_own.at[j], pg_peer.at[j], y_send, y_recv.at[j], (rep, fs_peer, tp))

    def a_copy(t, late):
        piece = ab.at[t, pl.ds(0, owned) if late else pl.ds(owned, 2 * owned)]
        k = blocks * late + t
        return remote(piece, piece, a_send, a_recv.at[k], (partner, fs, tp))

    def b_copy(kind, t):
        src = ab.at[t, pl.ds(owned, 2 * owned)] if kind == 0 else sb.at[t - blocks]
        return remote(src, bb.at[t], b_send, bc_recv.at[t], (far_mid, fs, tp))

    def last_copy(t, slot):
        rows = pl.ds(slot * owned, owned)
        recv = d_recv.at[t - items + 4] if slot else bc_recv.at[t]
        return remote(sb.at[t - blocks, rows], bb.at[t, rows], b_send, recv, (far_mid, fs, tp))

    def c_copy(t):
        return remote(
            bb.at[t, pl.ds(owned, owned)], bb.at[t, pl.ds(0, owned)], c_send, bc_recv.at[t], (partner, fs, tp)
        )

    half = tokens // n_fs
    own_half = pl.ds(pl.multiple_of(fs * half, 16), half)

    peer_half = pl.ds(pl.multiple_of(fs_peer * half, 16), half)

    def y_half(part):
        rows = own_half if part else peer_half
        return remote(
            pg_own.at[0, rows], pg_peer.at[0, rows], y_send, y_recv.at[blocks * part], (rep, fs_peer, tp)
        )

    def quarter_of(part):
        return pl.ds(pl.multiple_of(fs * half + part * (half // 2), 16), half // 2)

    def r_first(part):
        rows = quarter_of(part)
        return remote(
            right.at[blocks, rows], right_far.at[0, rows], r_send, r_recv.at[2 * blocks * part], (partner, fs, tp)
        )

    def f_first(part):
        piece = right_far.at[0, quarter_of(part)]
        return remote(piece, piece, f_send, f_recv.at[0], (rep, fs_peer, tp))

    def r_copy(q):
        return remote(
            right.at[blocks + q, own_half], right_far.at[q, own_half], r_send, r_recv.at[q], (partner, fs, tp)
        )

    def f_copy(q):
        piece = right_far.at[q, own_half]
        return remote(piece, piece, f_send, f_recv.at[q], (rep, fs_peer, tp))

    piece_rows = owned // n_tp

    def piece_of(slot, owner):
        return pl.ds(pl.multiple_of(slot * owned + owner * piece_rows, 16), piece_rows)

    def l_copy(slot):
        rows = piece_of(slot, tp)
        return remote(left.at[1, rows], left_far.at[rows], l_send, l_recv.at[slot], (partner, fs, tp))

    def m_copy(slot, hop):
        piece = left_far.at[piece_of(slot, tp_far if hop == 2 else tp)]
        k = 3 * slot + hop
        return remote(piece, piece, m_send, m_recv.at[k], (rep, fs, tp_next if hop else tp_far))

    def lanes(j):
        return pl.ds(pl.multiple_of(j * LANES, LANES), LANES)

    def term(kind, first, last, t):
        rows = slice(first * owned, last * owned)
        return jnp.dot(left[kind, rows, :], right[t], preferred_element_type=F32) * factor

    def long_term(first, last, t):
        rows = slice(first * owned, last * owned)
        own = jnp.dot(left[1, rows, :], right[t], preferred_element_type=F32)
        far = jnp.dot(left_far[rows, :], right_far[t - blocks], preferred_element_type=F32)
        return (own + far) * factor

    def loop(first, last, body):
        def step(i, carry):
            body(i)
            return carry
        lax.fori_loop(first, last, step, 0)

    def spread(kind, source):
        rows = CHUNK // 4
        lane = lax.broadcasted_iota(jnp.int32, (rows, CHUNK), 1)
        place = lax.broadcasted_iota(jnp.int32, (rows, CHUNK), 0) * 4
        pick = jnp.concatenate(
            [(place + owner == lane).astype(F32).astype(BF16) for owner in (mid, far_mid, far_end, end)], axis=0
        )
        for c in range(width // CHUNK):
            picked = lax.dot_general(
                pick, source[:, c * CHUNK:(c + 1) * CHUNK], NT, preferred_element_type=F32
            ).astype(BF16)
            for slot in range(4):
                left[kind, slot * owned + c * rows:slot * owned + (c + 1) * rows, :] = picked[slot * rows:(slot + 1) * rows]

    def item(kind, j):
        return j if kind == 0 else blocks + 2 * j + kind - 1

    def hidden_of(j):
        g = gate_ref[:, lanes(j)].astype(F32)
        u = up_ref[:, lanes(j)].astype(F32)
        right[j] = (g * (1.0 / (1.0 + jnp.exp(-g))) * u).astype(BF16)

    def send_down(t):
        ab[t] = term(0, 0, 3, t).astype(BF16)
        a_copy(t, 0).start()

    def partial_of(j):
        rows = pl.ds(pl.multiple_of(j * LANES, LANES), LANES)
        pg_own[j] = lax.dot_general(cot_ref[...], wd_ref[rows, :], NT, preferred_element_type=F32).astype(BF16)

    def partial_out(j):
        partial_of(j)
        y_copy(j).start()

    def grads_rows(j, rows):
        g = gate_ref[rows, lanes(j)].astype(F32)
        u = up_ref[rows, lanes(j)].astype(F32)
        total = pg_own[j, rows, :].astype(F32) + pg_peer[j, rows, :].astype(F32)
        s = 1.0 / (1.0 + jnp.exp(-g))
        t = blocks + 2 * j
        right[t, rows, :] = (total * u * s * (1.0 + g * (1.0 - s))).astype(BF16)
        right[t + 1, rows, :] = (total * (g * s)).astype(BF16)

    def grads_of(j):
        y_copy(j).wait_recv()
        grads_rows(j, slice(0, tokens))

    def finish(kind, j, piece):
        if kind == 0:
            dn_own[0:1, lanes(j)] = jnp.sum(piece * piece, axis=0, keepdims=True)
            down_out[pl.ds(pl.multiple_of(j * LANES, LANES), LANES), 0, :] = piece.T
        else:
            squares[kind - 1] += piece * piece
            (gate_out if kind == 1 else up_out)[:, 0, lanes(j)] = piece

    def down_on(t):
        a_copy(t, 0).wait_recv()
        rows = slice(owned, 3 * owned)
        ab[t, rows, :] = (ab[t, rows, :].astype(F32) + term(0, 1, 3, t)).astype(BF16)
        b_copy(0, t).start()

    def forward(q):
        r_copy(q).wait_recv()
        f_copy(q).start()

    def pair_on(kind, j):
        t = item(kind, j)
        f_copy(t - blocks).wait_recv()
        sb[t - blocks] = long_term(1, 3, t).astype(BF16)
        b_copy(kind, t).start()

    def settle(kind, j):
        t = item(kind, j)
        b_copy(kind, t).wait_recv()
        bb[t, owned:, :] = (bb[t, owned:, :].astype(F32) + term(min(kind, 1), 3, 4, t)).astype(BF16)
        c_copy(t).start()
        if kind:
            finish(kind, j, long_term(0, 1, t) + bb[t, :owned, :].astype(F32))

    def last_on(t):
        f_copy(t - blocks).wait_recv()
        sb[t - blocks] = long_term(1, 3, t).astype(BF16)
        last_copy(t, 1).start()

    def last_settle(t):
        last_copy(t, 1).wait_recv()
        bb[t, owned:, :] = (bb[t, owned:, :].astype(F32) + term(1, 3, 4, t)).astype(BF16)
        c_copy(t).start()

    def last_own(kind, j):
        t = item(kind, j)
        last_copy(t, 0).wait_recv()
        finish(kind, j, long_term(0, 1, t) + bb[t, :owned, :].astype(F32))

    def settle_own(j):
        a_copy(j, 1).wait_recv()
        finish(0, j, ab[j, :owned, :].astype(F32) + term(0, 0, 1, j) + bb[j, :owned, :].astype(F32))

    def last_hop(kind, j):
        t = item(kind, j)
        c_copy(t).wait_recv()
        finish(kind, j, bb[t, :owned, :].astype(F32) + term(min(kind, 1), 3, 4, t))

    def gi_term(j):
        t = blocks + 2 * j
        gi_acc[...] += lax.dot_general(right[t], wg_ref[:, lanes(j)], NT, preferred_element_type=F32) + lax.dot_general(
            right[t + 1], wu_ref[:, lanes(j)], NT, preferred_element_type=F32
        )

    def grads_and_term(j):
        grads_of(j)
        gi_term(j)

    def tokens_of(owner):
        return pl.ds(pl.multiple_of(owner * share, share), share)

    def gi_copy(step):
        other = lax.rem(tp + step, n_tp)
        return remote(
            gi_own.at[tokens_of(other)], gi_peer.at[step - 1], gi_send, gi_recv, in_tp(step)
        )

    def gg_copy(hop):
        piece = gi_ref.at[tokens_of(tp_far if hop == 2 else tp)]
        return remote(piece, piece, gg_send, gg_recv.at[hop], (rep, fs, tp_next if hop else tp_far))

    def gi_out():
        gi_own[...] = gi_acc[...].astype(BF16)
        for step in range(1, n_tp):
            gi_copy(step).start()

    here = (rep, fs_peer, tp)

    def all_in(whole, recv):
        remote(whole, whole, gi_send, recv, here).wait_recv()

    def all_out(whole, send):
        remote(whole, whole, send, gi_recv, here).wait_send()

    def gi_sum():
        all_in(gi_peer, gi_recv)
        whole = gi_own[tokens_of(tp), :].astype(F32)
        for step in range(1, n_tp):
            whole += gi_peer[step - 1].astype(F32)
        gi_ref[tokens_of(tp), :] = whole.astype(BF16)
        gg_copy(0).start()
        gg_copy(1).start()

    def gi_pass():
        gg_copy(0).wait_recv()
        gg_copy(2).start()

    def dn_copy(k):
        src = dn_sum.at[k] if k < 3 else dn_own
        place, other = ((1, (rep, fs_peer, tp)), (2, (far_mid, fs, tp)), (0, (partner, fs, tp)), (0, (partner, fs, tp)))[k]
        return remote(src, dn_peer.at[place], dn_send, dn_recv.at[place], other)

    def dn_on(k):
        dn_copy((3, 0, 1)[k]).wait_recv()
        dn_sum[k] = (dn_sum[k - 1] if k else dn_own[...]) + dn_peer[k]
        dn_copy(k).start()

    def gn_copy(step):
        return remote(gu_own, gu_peer.at[step - 1], gn_send, gn_recv, in_tp(step))

    def gn_out():
        for kind in range(2):
            gu_own[0:1, kind * owned:(kind + 1) * owned] = jnp.sum(squares[kind].T, axis=0, keepdims=True)
        for step in range(1, n_tp):
            gn_copy(step).start()

    loads[4].wait()
    load(2, 3)
    spread(1, x_ref)

    @pl.when(at_end)
    def _():
        pl.semaphore_wait(barrier, len(greeted))
        l_copy(1).start()
        l_copy(2).start()

    @pl.when(jnp.logical_not(at_end))
    def _():
        pl.semaphore_wait(barrier, len(greeted) + 1)

    loads[0].wait()
    loads[1].wait()
    load(7)
    loop(0, 1, partial_of)

    @pl.when(at_end)
    def _():
        y_half(0).start()
        y_half(1).start()

    @pl.when(jnp.logical_not(at_end))
    def _():
        y_copy(0).start()

    turn = blocks // 2

    def past(j, k):
        return jnp.where(j > k, 1, 0)

    def down_from(j):
        return jnp.minimum(j + 1 + past(j, turn) + past(j, turn + 2), blocks)

    def down_to(j):
        return jnp.minimum(j + 2 + past(j, turn - 1) + past(j, turn + 1), blocks)

    def late_to(j):
        return jnp.minimum(sum(jnp.maximum(j - LATE + k, 0) for k in (1, -1, -2, -3)), blocks)

    def sent_to(j):
        return jnp.minimum(j + AHEAD + past(j, 1), blocks)

    def grads_to(j):
        return jnp.minimum(j + AHEAD + past(j, 3), blocks)

    spread(0, cot_ref)
    loads[2].wait()
    loads[3].wait()
    load(5, 6)

    @pl.when(at_end)
    def _():
        def out(j):
            hidden_of(j)
            send_down(j)

        def pair_out(j):
            grads_of(j)
            r_copy(2 * j).start()
            r_copy(2 * j + 1).start()

        loop(0, 1, out)
        loop(1, AHEAD, partial_out)
        loads[7].wait()
        loop(AHEAD, 6, partial_out)
        gi_acc[...] = jnp.zeros_like(gi_acc)

        def both_out(j):
            pair_out(j)
            loop(down_from(j), down_to(j), out)

            @pl.when(j == 1)
            def _():
                l_copy(0).start()

            loop(late_to(j - 1), late_to(j), lambda t: a_copy(t, 1).start())

        y_half(0).wait_recv()
        grads_rows(0, own_half)
        r_first(0).start()
        r_first(1).start()
        r_copy(1).start()
        out(1)
        y_half(1).wait_recv()
        grads_rows(0, peer_half)
        loop(6, blocks, partial_out)
        loop(1, blocks, both_out)
        loop(late_to(blocks - 1), blocks, lambda t: a_copy(t, 1).start())
        squares[...] = jnp.zeros_like(squares)
        loads[5].wait()
        loads[6].wait()
        loop(0, blocks, gi_term)
        gi_out()

        def hops(j):
            loop(down_from(j - 2), down_to(j - 2), functools.partial(last_hop, 0))
            last_hop(1, j - 2)
            last_hop(2, j - 2)

        loop(0, 1, functools.partial(last_hop, 0))
        def pair_hops(j):
            last_hop(1, j)
            last_hop(2, j)

        loop(2, blocks - 3, hops)
        gi_sum()
        loop(down_from(blocks - 5), blocks, functools.partial(last_hop, 0))
        dn_copy(3).start()
        loop(blocks - 5, blocks - 3, pair_hops)
        gi_pass()
        loop(blocks - 3, blocks, pair_hops)
        gn_out()

    @pl.when(jnp.logical_not(at_end))
    def _():
        def spread_on(slot):
            l_copy(slot).wait_recv()
            m_copy(slot, 0).start()
            m_copy(slot, 1).start()

        def pass_on(slot):
            m_copy(slot, 0).wait_recv()
            m_copy(slot, 2).start()

        def landed(slot):
            m_copy(slot, 1).wait_recv()
            m_copy(slot, 2).wait_recv()

        def feed(j):
            forward(2 * j)
            forward(2 * j + 1)

            loop(sent_to(j - 1), sent_to(j), lambda k: y_copy(k).start())

        loop(1, 2, partial_out)
        loop(2, AHEAD, partial_of)
        loads[7].wait()
        loop(AHEAD, 8, partial_of)
        spread_on(1)
        loop(8, blocks, partial_of)
        loop(0, blocks, hidden_of)
        down_on(0)
        grads_of(0)
        spread_on(2)
        pass_on(1)
        gi_acc[...] = jnp.zeros_like(gi_acc)
        squares[...] = jnp.zeros_like(squares)
        for part in range(2):
            r_first(part).wait_recv()
            f_first(part).start()
        forward(1)
        loop(2, sent_to(0), lambda k: y_copy(k).start())
        pass_on(2)
        loads[5].wait()
        loads[6].wait()
        landed(1)
        landed(2)

        def step(j):
            pair_on(1, j)
            loop(down_from(j), down_to(j), down_on)
            pair_on(2, j)

            @pl.when(j + 1 < blocks)
            def _():
                feed(j + 1)

            @pl.when(j == 0)
            def _():
                gi_term(0)
                grads_and_term(1)

            loop(grads_to(j - 1), grads_to(j), grads_and_term)

        def settles(j):
            loop(down_from(j - 2), down_to(j - 2), functools.partial(settle, 0))
            settle(1, j - 2)
            settle(2, j - 2)
            loop(late_to(j - 2), late_to(j - 1), settle_own)

        loop(0, 2, step)
        spread_on(0)
        loop(0, 1, functools.partial(settle, 0))
        pass_on(0)
        step(2)
        landed(0)

        def both(j):
            settles(j - 1)
            step(j)

        loop(3, blocks - 3, both)
        gi_out()
        def pairs(j):
            settle(1, j)
            settle(2, j)

        def owns(j):
            last_own(1, j)
            last_own(2, j)

        loop(blocks - 3, blocks - 2, both)
        loop(items - 4, items - 2, last_on)
        feed(blocks - 1)
        loop(down_from(blocks - 5), blocks, functools.partial(settle, 0))
        loop(items - 2, items, last_on)
        loop(items - 4, items - 2, lambda t: last_copy(t, 0).start())
        loop(blocks - 5, blocks - 4, pairs)
        gi_sum()
        loop(blocks - 4, blocks - 3, pairs)
        loop(late_to(blocks - 5), blocks - 4, settle_own)
        loop(blocks - 3, blocks - 2, pairs)
        loop(blocks - 4, blocks, settle_own)
        loop(items - 4, items - 2, last_settle)
        dn_on(0)
        loop(items - 2, items, last_settle)
        gi_pass()
        dn_on(1)
        loop(items - 2, items, lambda t: last_copy(t, 0).start())
        loop(blocks - 2, blocks - 1, owns)
        dn_on(2)
        loop(blocks - 1, blocks, owns)
        gn_out()
        down_norm_ref[...] = dn_sum[2]

    @pl.when(at_end)
    def _():
        dn_copy(2).wait_recv()
        down_norm_ref[...] = dn_peer[0]

    gg_copy(1).wait_recv()
    gg_copy(2).wait_recv()
    all_out(gi_peer, gi_send)
    all_out(gi_ref.at[pl.ds(0, 3 * share)], gg_send)
    all_out(pg_peer, y_send)

    @pl.when(at_end)
    def _():
        all_out(left_far.at[pl.ds(0, 3 * piece_rows)], l_send)
        all_out(ab, a_send)
        all_out(dn_own, dn_send)
        all_out(right_far.at[:, own_half], r_send)

    @pl.when(jnp.logical_not(at_end))
    def _():
        all_out(left_far.at[pl.ds(0, 9 * piece_rows)], m_send)
        all_out(bb, b_send)
        all_out(dn_sum, dn_send)
        all_out(bb.at[:, pl.ds(0, owned)], c_send)
        all_out(right_far.at[:, own_half], f_send)

    all_in(gu_peer, gn_recv)
    gate_up = gu_own[...]
    for step in range(1, n_tp):
        gate_up += gu_peer[step - 1]
    gu_norm_ref[...] = gate_up
    all_out(gu_peer, gn_send)


def store_kernel(gi_ref, gate_ref, up_ref, down_ref, gu_ref, dn_ref, *rest):
    sem, line, outs = rest[-1], rest[-2], rest[:-2]
    owned = gu_ref.shape[1] // 2
    sources = (
        gate_ref, up_ref, down_ref, gi_ref, gu_ref.at[:, pl.ds(0, owned)], gu_ref.at[:, pl.ds(owned, owned)]
    )
    copies = [pltpu.make_async_copy(src, dst, sem.at[k]) for k, (src, dst) in enumerate(zip(sources, outs))]
    for copy in copies:
        copy.start()
    line[...] = dn_ref[0, :]
    for copy in copies:
        copy.wait()


def on_line(inputs, gate_pre, up_pre, cotangent, w_gate, w_up, w_down):
    n_fs, n_tp = lax.axis_size("fs"), lax.axis_size("tp")
    tokens, width = inputs.shape
    hunits = w_gate.shape[1]
    blocks = hunits // LANES
    items = 3 * blocks
    owned = width // 4
    share = tokens // n_tp
    dma = pltpu.SemaphoreType.DMA
    vmem = pltpu.VMEM
    sizes = (n_fs, n_tp, float(tokens * 4) ** (-0.5))
    shaped = jax.ShapeDtypeStruct
    gi_shape = shaped((tokens, width), BF16)
    row_shape = shaped((owned, 1, hunits), F32)
    down_shape = shaped((hunits, 1, owned), F32)
    results = pl.pallas_call(
        functools.partial(line_kernel, sizes),
        out_shape=(
            vmem((tokens, width), BF16),
            vmem((owned, 1, hunits), F32),
            vmem((owned, 1, hunits), F32),
            vmem((hunits, 1, owned), F32),
            vmem((1, 2 * owned), F32),
            vmem((1, hunits), F32),
        ),
        in_specs=[pl.BlockSpec(memory_space=pltpu.HBM)] * 7,
        out_specs=(pl.BlockSpec(memory_space=vmem),) * 6,
        scratch_shapes=[
            vmem((tokens, width), BF16),
            vmem((tokens, hunits), BF16),
            vmem((tokens, hunits), BF16),
            vmem((tokens, width), BF16),
            vmem((width, hunits), BF16),
            vmem((width, hunits), BF16),
            vmem((hunits, width), BF16),
            vmem((2, width, tokens), BF16),
            vmem((3 * owned, tokens), BF16),
            vmem((items, tokens, LANES), BF16),
            vmem((2 * blocks, tokens, LANES), BF16),
            vmem((blocks, tokens, LANES), BF16),
            vmem((blocks, tokens, LANES), BF16),
            vmem((blocks, 3 * owned, LANES), BF16),
            vmem((2 * blocks, 2 * owned, LANES), BF16),
            vmem((items, 2 * owned, LANES), BF16),
            vmem((tokens, width), F32),
            vmem((tokens, width), BF16),
            vmem((n_tp - 1, share, width), BF16),
            vmem((2, owned, LANES), F32),
            vmem((1, 2 * owned), F32),
            vmem((n_tp - 1, 1, 2 * owned), F32),
            vmem((1, hunits), F32),
            vmem((3, 1, hunits), F32),
            vmem((3, 1, hunits), F32),
            dma((8,)),
            dma((12,)),
            dma((blocks + 1,)),
            dma((2 * blocks,)),
            dma((items,)),
            dma((4,)),
            dma((2 * blocks + 1,)),
            dma((2 * blocks,)),
            dma((3,)),
            dma((9,)),
            dma((3,)),
            dma((2,)),
            dma((3,)),
        ],
        compiler_params=pltpu.CompilerParams(
            collective_id=0, has_side_effects=True, vmem_limit_bytes=VMEM_LIMIT
        ),
    )(inputs, gate_pre, up_pre, cotangent, w_gate, w_up, w_down)
    grad_gate, grad_up, grad_down, grad_input, gate_norms, up_norms, down_norms = pl.pallas_call(
        store_kernel,
        out_shape=(
            row_shape, row_shape, down_shape, gi_shape,
            shaped((1, owned), F32), shaped((1, owned), F32), shaped((hunits,), F32),
        ),
        in_specs=[pl.BlockSpec(memory_space=vmem)] * 6,
        out_specs=(pl.BlockSpec(memory_space=pltpu.HBM),) * 6 + (pl.BlockSpec(memory_space=vmem),),
        scratch_shapes=[dma((6,))],
        compiler_params=pltpu.CompilerParams(vmem_limit_bytes=2**23),
    )(*results)
    return (
        grad_input,
        grad_gate,
        grad_up,
        grad_down.transpose(0, 2, 1),
        gate_norms.reshape(owned, 1),
        up_norms.reshape(owned, 1),
        down_norms,
    )


def fits_line(mesh, inputs, w_gate):
    n_rep, n_fs, n_tp = (mesh.shape[axis] for axis in ("rep", "fs", "tp"))
    tokens, width = inputs.shape[0] // n_rep, inputs.shape[1] // n_fs
    return (
        n_rep == 4 and n_fs == 2 and n_tp == 4 and w_gate.shape[1] // n_tp >= 10 * LANES
        and width % (4 * LANES) == 0
        and tokens % (64 * n_fs) == 0 and tokens % LANES == 0
        and (w_gate.shape[1] // n_tp) % LANES == 0
    )


def solution(mesh):
    placed = (
        P("rep", "fs"),
        P("rep", "tp"),
        P("rep", "tp"),
        P("rep", None),
        P("fs", "tp"),
        P("fs", "tp"),
        P("tp", "fs"),
    )
    out_placed = (
        P("rep", "fs"),
        P("fs", "rep", "tp"),
        P("fs", "rep", "tp"),
        P("tp", "fs", "rep"),
        P("fs", "rep"),
        P("fs", "rep"),
        P("tp"),
    )

    def whole(inputs, gate_pre, up_pre, cotangent, w_gate, w_up, w_down):
        body = on_line if fits_line(mesh, inputs, w_gate) else on_device
        mapped = jax.shard_map(body, mesh=mesh, in_specs=placed, out_specs=out_placed, check_vma=False)
        return mapped(inputs, gate_pre, up_pre, cotangent, w_gate, w_up, w_down)

    return whole
```
